32 devices in a mesh: sp: 8 (over z, x), tp: 4 (over y, core).
Axes of the slice: x: 2, y: 2, z: 4, core: 2. Of those that a mesh axis runs over, the one named last changes fastest.
Arguments:
- tokens: bfloat16 [4096, 2048], P('sp', 'tp'), may hold values from -6 to 6
- norm_gain: float32 [2048], replicated, may hold values from 0.1 to 1.9
- proj_state: bfloat16 [2048, 1024], P('sp', 'tp'), may hold values from -0.125 to 0.125
- proj_value: bfloat16 [2048, 1024], P('sp', 'tp'), may hold values from -0.125 to 0.125
- proj_gate: bfloat16 [2048, 1024], P('sp', 'tp'), may hold values from -0.125 to 0.125
- eigen_real: float32 [64, 64], P('tp')
- eigen_imag: float32 [64, 64], P('tp')
- log_step: float32 [64], P('tp')
- decay_shift: float32 [64, 4096], P('tp', 'sp'), may hold values from -2.2 to 0
- state_input: float32 [2, 64, 16, 64], P(None, 'tp'), may hold values from -1 to 1
- state_readout_matrices: float32 [2, 64, 16, 64], P(None, 'tp'), may hold values from -0.5 to 0.5
- skip_gain: float32 [1024], P('tp'), may hold values from -5 to 5
- init_state: float32 [2, 64, 64], P(None, 'tp'), may hold values from -5 to 5
- conv_taps: float32 [31, 1024], P(None, 'tp')
- channel_gain: float32 [1024], P('tp'), may hold values from 0.1 to 1.9
- merge_state: bfloat16 [1024, 2048], P('tp', 'sp'), may hold values from -0.125 to 0.125
- merge_conv: bfloat16 [1024, 2048], P('tp', 'sp'), may hold values from -0.125 to 0.125
Outputs:
- mixed: bfloat16 [4096, 2048], P(('sp', 'tp'))
The draws below stay inside these ranges and needn't reach their ends.
All inputs are finite; a program needn't handle non-finite values.
Results may differ from the reference program's by a relative error of at most 0.011.
Values may be sent and summed in bfloat16 or wider, within the bound.
A program may use at most 128 MiB of HBM per device.

```python
import math
import jax
import jax.numpy as jnp
from jax import lax

D = 2048
SSM_W = 1024
GROUP = 16
STATE = 64
CONV_W = 1024
KERNEL = 31
TOK_DEV = 512
GROUPS = 64
TOKENS = 4096
N_TP = 4


def speeds(key):
    base = jax.random.fold_in(key, 101)
    first, second, third = jax.random.split(base, 3)
    fast = jax.random.randint(first, (GROUPS,), 0, 2) == 0
    reach = jax.random.uniform(second, (GROUPS,), jnp.float32, 30.0, 100.0)
    rate = jnp.where(fast, 0.5 / reach, 0.2 / TOKENS)
    step = 2.0 * jnp.sqrt(2.0 * rate) * jax.random.uniform(third, (GROUPS,), jnp.float32, 0.7, 1.4)
    return (rate, step)


def draw_log_step(key, part):
    rate, step = speeds(key)
    return jnp.log(step).astype(jnp.float32)


def draw_eigen_real(key, part):
    rate, step = speeds(key)
    factor = jax.random.uniform(jax.random.fold_in(key, 202), (GROUPS, STATE), jnp.float32, 0.8, 1.25)
    return (-rate[:, None] * factor / step[:, None]).astype(jnp.float32)


def draw_eigen_imag(key, part):
    rate, step = speeds(key)
    first, second = jax.random.split(jax.random.fold_in(key, 303))
    angle = jax.random.uniform(first, (GROUPS, STATE), jnp.float32, 0.05, 0.4)
    signs = (2 * jax.random.randint(second, (GROUPS, STATE), 0, 2) - 1).astype(jnp.float32)
    return (signs * angle / step[:, None]).astype(jnp.float32)


def draw_decay_shift(key, part):
    rate, step = speeds(key)
    first, second, third = jax.random.split(jax.random.fold_in(key, 404), 3)
    factor = jax.random.uniform(first, (GROUPS, TOKENS // 32), jnp.float32, 0.0, 2.0)
    shift = -rate[:, None] * jnp.repeat(factor, 32, axis=1, total_repeat_length=TOKENS)
    places = jax.random.randint(second, (GROUPS, 3), 0, TOKENS)
    depth = jax.random.uniform(third, (GROUPS, 3), jnp.float32, 0.22, 0.69)
    rows_index = jnp.broadcast_to(jnp.arange(GROUPS)[:, None], (GROUPS, 3))
    shift = shift.at[rows_index, places].add(-depth)
    return shift.astype(jnp.float32)


def draw_conv_taps(key, part):
    first, second = jax.random.split(jax.random.fold_in(key, 505))
    place = jnp.arange(CONV_W).astype(jnp.float32) / max(CONV_W - 1, 1)
    noise = jax.random.normal(first, (KERNEL, CONV_W), jnp.float32)
    ramp = jnp.exp(math.log(3.0) * place)
    scale = jnp.exp(jax.random.uniform(second, (CONV_W,), jnp.float32, 0.0, math.log(10.0)))
    return (noise * scale * ramp / math.sqrt(KERNEL)).astype(jnp.float32)


def levels(own_key, extent, cuts, least, largest):
    level = 1.0
    for axis_at, parts in cuts:
        heights = jax.random.uniform(jax.random.fold_in(jax.random.fold_in(own_key, 6), axis_at), (parts,), jnp.float32, least / len(cuts), largest / len(cuts))
        level = level * jnp.repeat(jnp.exp(heights), extent[axis_at] // parts).reshape((-1,) + (1,) * (len(extent) - 1 - axis_at))
    return level


def bell_draw(stream_key, dims, width, most, shards=(), held_as=jnp.bfloat16):
    factor_of = levels(stream_key, dims, shards, -0.22, 0.18) if shards else 1.0
    array = jax.random.normal(stream_key, dims, jnp.float32) * width * factor_of
    return jnp.minimum(jnp.maximum(array, -most), most).astype(held_as)


def setup_inputs(seed: int = 0) -> dict:
    splits = jax.random.split(jax.random.key(seed), 18)
    tokens = bell_draw(splits[0], (TOKENS, D), 1.0, 6.0, ((0, 8), (1, 4)))
    norm_gain = jnp.clip(1.0 + 0.18 * jax.random.normal(splits[1], (D,), jnp.float32), 0.1, 1.9)
    proj_state = bell_draw(splits[2], (D, SSM_W), D ** -0.5, 0.125, ((0, 8), (1, 4)))
    proj_value = bell_draw(splits[3], (D, CONV_W), D ** -0.5, 0.125, ((0, 8), (1, 4)))
    proj_gate = bell_draw(splits[4], (D, CONV_W), D ** -0.5, 0.125, ((0, 8), (1, 4)))
    eigen_real = draw_eigen_real(jax.random.fold_in(splits[17], 71), 0)
    eigen_imag = draw_eigen_imag(jax.random.fold_in(splits[17], 71), 0)
    log_step = draw_log_step(jax.random.fold_in(splits[17], 71), 0)
    decay_shift = draw_decay_shift(jax.random.fold_in(splits[17], 71), 0)
    state_input = bell_draw(splits[9], (2, GROUPS, GROUP, STATE), 0.18, 1.0, ((1, 4),), jnp.float32)
    state_readout_matrices = bell_draw(splits[10], (2, GROUPS, GROUP, STATE), 0.09, 0.5, ((1, 4),), jnp.float32)
    skip_gain = bell_draw(splits[11], (SSM_W,), 1.0, 5.0, ((0, 4),), jnp.float32)
    init_state = bell_draw(splits[12], (2, GROUPS, STATE), 1.0, 5.0, ((1, 4),), jnp.float32)
    conv_taps = draw_conv_taps(jax.random.fold_in(splits[17], 71), 0)
    channel_gain = jnp.clip(1.0 + 0.18 * jax.random.normal(splits[14], (CONV_W,), jnp.float32), 0.1, 1.9)
    merge_state = bell_draw(splits[15], (SSM_W, D), (SSM_W + CONV_W) ** -0.5, 0.125, ((0, 4), (1, 8)))
    merge_conv = bell_draw(splits[16], (CONV_W, D), (SSM_W + CONV_W) ** -0.5, 0.125, ((0, 4), (1, 8)))
    return {"tokens": tokens, "norm_gain": norm_gain, "proj_state": proj_state, "proj_value": proj_value, "proj_gate": proj_gate, "eigen_real": eigen_real, "eigen_imag": eigen_imag, "log_step": log_step, "decay_shift": decay_shift, "state_input": state_input, "state_readout_matrices": state_readout_matrices, "skip_gain": skip_gain, "init_state": init_state, "conv_taps": conv_taps, "channel_gain": channel_gain, "merge_state": merge_state, "merge_conv": merge_conv}


epsilon = 1e-06
exact_precision = lax.Precision.HIGHEST

def round_half(value):
    return lax.optimization_barrier(value.astype(jnp.bfloat16))

def input_matrix(eigen_real, eigen_imag, step, state_input):
    base = eigen_real * step[:, None]
    theta = eigen_imag * step[:, None]
    magnitude = jnp.exp(base)
    near_re = magnitude * jnp.cos(theta) - 1.0
    near_im = magnitude * jnp.sin(theta)
    modulus = eigen_real * eigen_real + eigen_imag * eigen_imag
    ratio_re = (near_re * eigen_real + near_im * eigen_imag) / modulus
    ratio_im = (near_im * eigen_real - near_re * eigen_imag) / modulus
    in_re = state_input[0]
    in_im = state_input[1]
    discrete_decay_real = ratio_re[:, None, :] * in_re - ratio_im[:, None, :] * in_im
    discrete_decay_imaginary = ratio_re[:, None, :] * in_im + ratio_im[:, None, :] * in_re
    return (discrete_decay_real, discrete_decay_imaginary)

def block_states(c_re, c_im, delta_real, delta_imaginary, shift, base, theta, counts, lower):
    level = jnp.cumsum(shift, axis=0)[:, :, None] + counts * base
    angle = counts * theta
    cosine = jnp.cos(angle)
    sine = jnp.sin(angle)
    grow = jnp.exp(level)
    shrink = jnp.exp(-level)
    w_re = shrink * (cosine * delta_real + sine * delta_imaginary)
    w_im = shrink * (cosine * delta_imaginary - sine * delta_real)
    length, groups, states = delta_real.shape
    stacked = jnp.concatenate([w_re, w_im], axis=1).reshape(length, 2 * groups * states)
    summed = jnp.dot(lower, stacked, precision=exact_precision).reshape(length, 2 * groups, states)
    t_re = summed[:, :groups] + c_re
    t_im = summed[:, groups:] + c_im
    input_real = grow * (cosine * t_re - sine * t_im)
    input_imaginary = grow * (cosine * t_im + sine * t_re)
    return (input_real, input_imaginary)

def state_branch(u_in, eigen_real, eigen_imag, log_step, decay_shift, state_input, state_readout_matrices, skip_gain, init_state):
    step = jnp.exp(log_step)
    base = eigen_real * step[:, None]
    theta = eigen_imag * step[:, None]
    discrete_decay_real, discrete_decay_imaginary = input_matrix(eigen_real, eigen_imag, step, state_input)
    length = min(32, TOK_DEV)
    blocks = TOKENS // length
    values = u_in.reshape(blocks, length, GROUPS, GROUP)
    shifts = decay_shift.T.reshape(blocks, length, GROUPS)
    counts = (jnp.arange(length) + 1).astype(jnp.float32)[:, None, None]
    lower = (jnp.arange(length)[:, None] >= jnp.arange(length)[None, :]).astype(jnp.float32)
    output_real = state_readout_matrices[0]
    output_imaginary = state_readout_matrices[1]
    skips = skip_gain.reshape(GROUPS, GROUP)

    def advance(carry, inputs):
        block_u, block_shift = inputs
        float_values = block_u.astype(jnp.float32)
        delta_real = jnp.einsum('ovi,viu->ovu', float_values, discrete_decay_real, precision=exact_precision)
        delta_imaginary = jnp.einsum('ovi,viu->ovu', float_values, discrete_decay_imaginary, precision=exact_precision)
        input_real, input_imaginary = block_states(carry[0], carry[1], delta_real, delta_imaginary, block_shift, base, theta, counts, lower)
        final_output = jnp.einsum('lan,arn->lar', input_real, output_real, precision=exact_precision) - jnp.einsum('lan,arn->lar', input_imaginary, output_imaginary, precision=exact_precision)
        final_output = final_output + skips * float_values
        return ((input_real[-1], input_imaginary[-1]), jax.nn.gelu(final_output).astype(jnp.bfloat16))
    start = (init_state[0].astype(jnp.float32), init_state[1].astype(jnp.float32))
    _, outs = lax.scan(advance, start, (values, shifts))
    return outs.reshape(TOKENS, SSM_W)

def conv_branch(value, gate, conv_taps, channel_gain):
    glu = round_half(value.astype(jnp.float32) * jax.nn.sigmoid(gate.astype(jnp.float32)))
    reach = KERNEL - 1
    count = glu.shape[0]
    extended = jnp.concatenate([jnp.zeros((reach, CONV_W), jnp.bfloat16), glu], axis=0).astype(jnp.float32)
    raw = jnp.zeros((count, CONV_W), jnp.float32)
    for offset in range(KERNEL):
        raw = raw + conv_taps[offset] * extended[offset:offset + count]
    first = lax.optimization_barrier(jnp.sum(raw, axis=1, keepdims=True))
    second = lax.optimization_barrier(jnp.sum(raw * raw, axis=1, keepdims=True))
    middle = first / CONV_W
    spread = second / CONV_W - middle * middle
    scaled = (raw - middle) * lax.rsqrt(spread + epsilon) * channel_gain
    return jax.nn.silu(scaled).astype(jnp.bfloat16)

def reference(tokens, norm_gain, proj_state, proj_value, proj_gate, eigen_real, eigen_imag, log_step, decay_shift, state_input, state_readout_matrices, skip_gain, init_state, conv_taps, channel_gain, merge_state, merge_conv):
    wide = tokens.astype(jnp.float32)
    normed = (wide * lax.rsqrt(lax.optimization_barrier(jnp.mean(wide * wide, axis=1, keepdims=True)) + epsilon) * norm_gain).astype(jnp.bfloat16)
    u_in = round_half(jnp.dot(normed, proj_state, preferred_element_type=jnp.float32))
    value = round_half(jnp.dot(normed, proj_value, preferred_element_type=jnp.float32))
    gate = round_half(jnp.dot(normed, proj_gate, preferred_element_type=jnp.float32))
    ssm_out = state_branch(u_in, eigen_real, eigen_imag, log_step, decay_shift, state_input, state_readout_matrices, skip_gain, init_state)
    conv_out = conv_branch(value, gate, conv_taps, channel_gain)
    state_part = SSM_W // N_TP
    conv_part = CONV_W // N_TP
    total = jnp.zeros((TOKENS, D), jnp.float32)
    for index in range(N_TP):
        term = jnp.dot(ssm_out[:, index * state_part:(index + 1) * state_part], merge_state[index * state_part:(index + 1) * state_part], preferred_element_type=jnp.float32)
        term = term + jnp.dot(conv_out[:, index * conv_part:(index + 1) * conv_part], merge_conv[index * conv_part:(index + 1) * conv_part], preferred_element_type=jnp.float32)
        total = total + round_half(term).astype(jnp.float32)
    return total.astype(jnp.bfloat16)
```

```python
import functools

import jax
import jax.numpy as jnp
from jax import lax
from jax.experimental import pallas as pl
from jax.experimental.pallas import tpu as pltpu
from jax.sharding import PartitionSpec as P

CONV_W = 1024


epsilon = 1e-06
exact_precision = lax.Precision.HIGHEST


def entering(value, axis, join, neutral):
    count, mine = (lax.axis_size(axis), lax.axis_index(axis))
    pieces = jax.tree.map(lambda part: lax.all_gather(part, axis), value)
    total = jax.tree.map(
        lambda part, zero: jnp.full_like(part, 0) + jnp.asarray(zero, part.dtype), value, neutral
    )

    def hop(position, total):
        longer = join(total, jax.tree.map(lambda part: part[position], pieces))
        return jax.tree.map(lambda new, old: jnp.where(position < mine, new, old), longer, total)

    return lax.fori_loop(0, count - 1, hop, total)


def passed_along(block, axis, distance):
    devices = range(lax.axis_size(axis))
    route = [(i - distance, i) for i in devices if i - distance in devices]
    return lax.ppermute(block, axis, route)


def round_half(value):
    return lax.optimization_barrier(value.astype(jnp.bfloat16))


def input_matrix(eigen_real, eigen_imag, step, state_input):
    base = eigen_real * step[:, None]
    theta = eigen_imag * step[:, None]
    magnitude = jnp.exp(base)
    near_re = magnitude * jnp.cos(theta) - 1.0
    near_im = magnitude * jnp.sin(theta)
    modulus = eigen_real * eigen_real + eigen_imag * eigen_imag
    ratio_re = (near_re * eigen_real + near_im * eigen_imag) / modulus
    ratio_im = (near_im * eigen_real - near_re * eigen_imag) / modulus
    in_re = state_input[0]
    in_im = state_input[1]
    discrete_decay_real = ratio_re[:, None, :] * in_re - ratio_im[:, None, :] * in_im
    discrete_decay_imaginary = ratio_re[:, None, :] * in_im + ratio_im[:, None, :] * in_re
    return (discrete_decay_real, discrete_decay_imaginary)


def block_states(c_re, c_im, delta_real, delta_imaginary, shift, base, theta, counts, lower):
    level = jnp.cumsum(shift, axis=0)[:, :, None] + counts * base
    angle = counts * theta
    cosine = jnp.cos(angle)
    sine = jnp.sin(angle)
    grow = jnp.exp(level)
    shrink = jnp.exp(-level)
    w_re = shrink * (cosine * delta_real + sine * delta_imaginary)
    w_im = shrink * (cosine * delta_imaginary - sine * delta_real)
    length, groups, states = delta_real.shape
    stacked = jnp.concatenate([w_re, w_im], axis=1).reshape(length, 2 * groups * states)
    summed = jnp.dot(lower, stacked, precision=exact_precision).reshape(length, 2 * groups, states)
    t_re = summed[:, :groups] + c_re
    t_im = summed[:, groups:] + c_im
    input_real = grow * (cosine * t_re - sine * t_im)
    input_imaginary = grow * (cosine * t_im + sine * t_re)
    return (input_real, input_imaginary)


def chain(earlier, later):
    a_re, a_im, b_re, b_im = earlier
    c_re, c_im, delta_real, delta_imaginary = later
    return (
        a_re * c_re - a_im * c_im,
        a_re * c_im + a_im * c_re,
        c_re * b_re - c_im * b_im + delta_real,
        c_re * b_im + c_im * b_re + delta_imaginary,
    )


def state_local(
    u_in, eigen_real, eigen_imag, log_step, decay_shift, state_input, state_readout_matrices
):
    count, width = u_in.shape
    groups, states = eigen_real.shape
    group = width // groups
    step = jnp.exp(log_step)
    base = eigen_real * step[:, None]
    theta = eigen_imag * step[:, None]
    discrete_decay_real, discrete_decay_imaginary = input_matrix(
        eigen_real, eigen_imag, step, state_input
    )
    float_values = u_in.astype(jnp.float32).reshape(count, groups, group)
    forcing_real = jnp.einsum(
        "ovi,viu->ovu", float_values, discrete_decay_real, precision=exact_precision
    )
    forcing_imaginary = jnp.einsum(
        "ovi,viu->ovu", float_values, discrete_decay_imaginary, precision=exact_precision
    )
    shift = decay_shift.T
    length = min(32, count)
    blocks = count // length
    counts = (jnp.arange(length) + 1).astype(jnp.float32)[:, None, None]
    lower = (jnp.arange(length)[:, None] >= jnp.arange(length)[None, :]).astype(jnp.float32)

    def advance(carry, inputs):
        delta_real, delta_imaginary, block_shift = inputs
        input_real, input_imaginary = block_states(
            carry[0], carry[1], delta_real, delta_imaginary, block_shift, base, theta, counts, lower
        )
        return ((input_real[-1], input_imaginary[-1]), (input_real, input_imaginary))

    zero = jnp.zeros((groups, states), jnp.float32)
    last, (input_real, input_imaginary) = lax.scan(
        advance,
        (zero, zero),
        (
            forcing_real.reshape(blocks, length, groups, states),
            forcing_imaginary.reshape(blocks, length, groups, states),
            shift.reshape(blocks, length, groups),
        ),
    )
    input_real = input_real.reshape(count, groups, states)
    input_imaginary = input_imaginary.reshape(count, groups, states)
    local_output = jnp.einsum(
        "lan,arn->lar", input_real, state_readout_matrices[0], precision=exact_precision
    ) - jnp.einsum(
        "lan,arn->lar", input_imaginary, state_readout_matrices[1], precision=exact_precision
    )
    whole_count = (jnp.arange(count) + 1).astype(jnp.float32)[:, None, None]
    level = jnp.cumsum(shift, axis=0)[:, :, None] + whole_count * base
    angle = whole_count * theta
    grow = jnp.exp(level)
    exponent_real = grow * jnp.cos(angle)
    exponent_imaginary = grow * jnp.sin(angle)
    summary = (exponent_real[-1], exponent_imaginary[-1], last[0], last[1])
    return (local_output, exponent_real, exponent_imaginary, summary)


def carry_in(summary, init_state):
    groups, states = summary[0].shape
    ones = jnp.ones((groups, states), jnp.float32)
    zeros = jnp.zeros((groups, states), jnp.float32)
    identity = (ones, zeros, zeros, zeros)
    before = entering(summary, "sp", chain, identity)
    a_re, a_im, b_re, b_im = before
    s_re = init_state[0]
    s_im = init_state[1]
    return (a_re * s_re - a_im * s_im + b_re, a_re * s_im + a_im * s_re + b_im)


def state_finish(
    local_output,
    exponent_real,
    exponent_imaginary,
    carried,
    state_readout_matrices,
    skip_gain,
    u_in,
):
    h_re, h_im = carried
    output_real = state_readout_matrices[0]
    output_imaginary = state_readout_matrices[1]
    blend_real = output_real * h_re[:, None, :] - output_imaginary * h_im[:, None, :]
    blend_imaginary = output_real * h_im[:, None, :] + output_imaginary * h_re[:, None, :]
    total = (
        local_output
        + jnp.einsum("lan,arn->lar", exponent_real, blend_real, precision=exact_precision)
        - jnp.einsum("lan,arn->lar", exponent_imaginary, blend_imaginary, precision=exact_precision)
    )
    count, width = u_in.shape
    groups = local_output.shape[1]
    float_values = u_in.astype(jnp.float32).reshape(count, groups, width // groups)
    total = total + skip_gain.reshape(groups, width // groups) * float_values
    return jax.nn.gelu(total).reshape(count, width).astype(jnp.bfloat16)


def conv_branch(value, gate, conv_taps, channel_gain):
    glu = round_half(value.astype(jnp.float32) * jax.nn.sigmoid(gate.astype(jnp.float32)))
    reach = conv_taps.shape[0] - 1
    count = glu.shape[0]
    before = passed_along(glu[count - reach :], "sp", 1)
    extended = jnp.concatenate([before, glu], axis=0).astype(jnp.float32)
    raw = jnp.zeros(glu.shape, jnp.float32)
    for offset in range(reach + 1):
        raw = raw + conv_taps[offset] * extended[offset : offset + count]
    first, second = lax.psum(
        (jnp.sum(raw, axis=1, keepdims=True), jnp.sum(raw * raw, axis=1, keepdims=True)), "tp"
    )
    middle = first / CONV_W
    spread = second / CONV_W - middle * middle
    scaled = (raw - middle) * lax.rsqrt(spread + epsilon) * channel_gain
    return jax.nn.silu(scaled).astype(jnp.bfloat16)


def per_device(
    tokens,
    norm_gain,
    proj_state,
    proj_value,
    proj_gate,
    eigen_real,
    eigen_imag,
    log_step,
    decay_shift,
    state_input,
    state_readout_matrices,
    skip_gain,
    init_state,
    conv_taps,
    channel_gain,
    merge_state,
    merge_conv,
):
    whole = lax.all_gather(tokens, "tp", axis=1, tiled=True)
    wide = whole.astype(jnp.float32)
    normed = (
        wide * lax.rsqrt(jnp.mean(wide * wide, axis=1, keepdims=True) + epsilon) * norm_gain
    ).astype(jnp.bfloat16)
    pieces = (
        lax.all_gather(proj_state, "sp", axis=0, tiled=True),
        lax.all_gather(proj_value, "sp", axis=0, tiled=True),
        lax.all_gather(proj_gate, "sp", axis=0, tiled=True),
    )
    state_sum, value_sum, gate_sum = tuple(
        (jnp.dot(normed, piece, preferred_element_type=jnp.float32) for piece in pieces)
    )
    u_in = round_half(state_sum)
    local_output, exponent_real, exponent_imaginary, summary = state_local(
        u_in, eigen_real, eigen_imag, log_step, decay_shift, state_input, state_readout_matrices
    )
    carried = carry_in(summary, init_state)
    conv_out = conv_branch(round_half(value_sum), round_half(gate_sum), conv_taps, channel_gain)
    ssm_out = state_finish(
        local_output,
        exponent_real,
        exponent_imaginary,
        carried,
        state_readout_matrices,
        skip_gain,
        u_in,
    )
    full_state, full_conv = (
        lax.all_gather(merge_state, "sp", axis=1, tiled=True),
        lax.all_gather(merge_conv, "sp", axis=1, tiled=True),
    )
    return lax.psum_scatter(
        (
            jnp.dot(ssm_out, full_state, preferred_element_type=jnp.float32)
            + jnp.dot(conv_out, full_conv, preferred_element_type=jnp.float32)
        ).astype(jnp.bfloat16),
        "tp",
        scatter_dimension=0,
        tiled=True,
    )


MESH = pl.DeviceIdType.MESH
F32 = jnp.float32
BF16 = jnp.bfloat16
BLOCK = 32


def dot(a, b):
    return jnp.dot(a, b, preferred_element_type=F32)


def dot_exact(a, b):
    return jnp.dot(a, b, preferred_element_type=F32, precision=exact_precision)


def split(value):
    high = value.astype(BF16)
    return high, (value - high.astype(F32)).astype(BF16)


def ring_position(index, n):
    return jnp.where(index % 2 == 0, index // 2, n - 1 - index // 2)


def ring_index(position, n):
    position = lax.rem(position + 2 * n, n)
    return jnp.where(position < n // 2, 2 * position, 2 * (n - 1 - position) + 1)


def mixer_kernel(
    n, ntp,
    tokens, gain, proj_s, proj_v, proj_g, shift, expand, base_t, cos_t, sin_t,
    binp, cout, skip, init, taps, chgain, merge_s, merge_c,
    out,
    tok, normed, gat, mgat, u_buf, forc, grow_buf, xs, ext, raw, ssm, conv,
    halo, glu_tail, summ, summ_in, stat, stat_in, snd, own, rp, s2, r2,
    loc_sem, tok_s, tok_r, fwd_s, fwd_r, ring_s, ring_r, halo_s, halo_r,
    sum_s, sum_r, st_s, st_r, rp_s, rp_r, r2_s, r2_r,
):
    sp = lax.axis_index("sp")
    tp = lax.axis_index("tp")
    ny = ntp // 2
    y, core = tp // 2, tp % 2
    partner = y * 2 + 1 - core
    pos = ring_position(sp, n)
    right, left = ring_index(pos + 1, n), ring_index(pos - 1, n)
    count, width = u_buf.shape
    lanes = grow_buf.shape[1]
    part = tokens.shape[1]
    rows_w = proj_s.shape[0]

    halo[...] = jnp.zeros_like(halo)
    summ_in[...] = jnp.zeros_like(summ_in)

    barrier = pltpu.get_barrier_semaphore()
    for d in range(1, n):
        pl.semaphore_signal(barrier, inc=1, device_id=(lax.rem(sp + d, n), tp), device_id_type=MESH)
    for d in range(1, ntp):
        pl.semaphore_signal(barrier, inc=1, device_id=(sp, lax.rem(tp + d, ntp)), device_id_type=MESH)
    pl.semaphore_wait(barrier, n + ntp - 2)

    def remote(src, dst, s, r, where):
        return pltpu.make_async_remote_copy(
            src_ref=src, dst_ref=dst, send_sem=s, recv_sem=r, device_id=where, device_id_type=MESH
        )

    sources = (proj_s, proj_v, proj_g, merge_s, merge_c)
    hops = n // 2

    def slot(w, origin):
        return gat.at[w, origin] if w < 3 else mgat.at[w - 3, origin]

    def piece(w, side, step):
        origin = ring_index(pos - step if side == 0 else pos + step, n)
        where = (right if side == 0 else left, tp)
        src = sources[w] if step == 0 else slot(w, origin)
        dst = slot(w, origin)
        if step == hops - 1:
            half = src.shape[0] // 2
            window = pl.ds(side * half, half)
            src, dst = src.at[window], dst.at[window]
        return remote(src, dst, ring_s.at[w, side, step], ring_r.at[w, side, step], where)

    def ring_send(ws, step):
        for w in ws:
            for side in range(2):
                if step > 0:
                    piece(w, side, step - 1).wait_recv()
                piece(w, side, step).start()

    def ring_end(ws):
        for w in ws:
            for side in range(2):
                piece(w, side, hops - 1).wait_recv()

    proj_set, merge_set = range(3), range(3, 5)
    ring_send(proj_set, 0)

    def tok_copy(d):
        where = (sp, lax.rem(y + d, ny) * 2 + core) if d else (sp, partner)
        return remote(tokens, tok.at[tp], tok_s.at[d], tok_r.at[d], where)

    def tok_forward(d):
        origin = lax.rem(y - d + ny, ny) * 2 + core
        return remote(tok.at[origin], tok.at[origin], fwd_s.at[d], fwd_r.at[d], (sp, partner))

    for d in list(range(1, ny)) + [0]:
        tok_copy(d).start()
    local = [pltpu.make_async_copy(tokens, tok.at[tp], loc_sem.at[5])]
    for w in range(5):
        local.append(pltpu.make_async_copy(sources[w], slot(w, sp), loc_sem.at[w]))
    for c in local:
        c.start()
    ring_send(proj_set, 1)
    for d in range(1, ny):
        tok_copy(d).wait_recv()
        tok_forward(d).start()
    tok_copy(0).wait_recv()
    for c in local:
        c.wait()
    for step in range(2, hops - 1):
        ring_send(proj_set, step)
    for d in range(1, ny):
        tok_forward(d).wait_recv()

    tile = 64

    @pl.loop(0, count // tile)
    def _(i):
        rows = pl.ds(pl.multiple_of(i * tile, tile), tile)
        pieces = [tok[j, rows, :].astype(F32) for j in range(ntp)]
        square = sum(jnp.sum(p * p, axis=1, keepdims=True) for p in pieces)
        scale = lax.rsqrt(square / (part * ntp) + epsilon)
        for j in range(ntp):
            cols = slice(j * part, (j + 1) * part)
            normed[rows, cols] = (pieces[j] * scale * gain[:, cols]).astype(BF16)

    ring_send(proj_set, hops - 1)
    ring_send(merge_set, 0)
    ring_end(proj_set)

    big = 128

    def project(w, i):
        rows = pl.ds(pl.multiple_of(i * big, big), big)
        total = dot(normed[rows, 0:rows_w], gat[w, 0])
        for o in range(1, n):
            total += dot(normed[rows, o * rows_w : (o + 1) * rows_w], gat[w, o])
        return rows, total.astype(BF16)

    @pl.loop(0, count // big)
    def _(i):
        rows, value = project(1, i)
        rows, gate = project(2, i)
        glu = (value.astype(F32) * jax.nn.sigmoid(gate.astype(F32))).astype(BF16)
        ext[pl.ds(pl.multiple_of(BLOCK + i * big, BLOCK), big), :] = glu.astype(F32)
        rows, u = project(0, i)
        u_buf[rows, :] = u

    ring_send(merge_set, 1)
    glu_tail[...] = ext[count : count + BLOCK, :].astype(BF16)
    halo_to = lax.rem(sp + 1, n)
    halo_copy = remote(glu_tail, halo, halo_s, halo_r, (halo_to, tp))

    @pl.when(sp < n - 1)
    def _():
        halo_copy.start()

    wide = 256

    @pl.loop(0, 2 * lanes // wide)
    def _(j):
        cols = pl.ds(pl.multiple_of(j * wide, wide), wide)
        high, low = split(binp[:, cols])
        forc[:, cols] = dot(u_buf[...], high) + dot(u_buf[...], low)

    row_i = lax.broadcasted_iota(jnp.int32, (BLOCK, BLOCK), 0)
    col_i = lax.broadcasted_iota(jnp.int32, (BLOCK, BLOCK), 1)
    lower = (row_i >= col_i).astype(F32)
    last = slice(BLOCK - 1, BLOCK)

    def first_pass(k, state):
        a_re, a_im, c_re, c_im = state
        rows = pl.ds(pl.multiple_of(k * BLOCK, BLOCK), BLOCK)
        level = dot_exact(dot_exact(lower, shift[rows, :]), expand[...]) + base_t[...]
        grow, shrink = jnp.exp(level), jnp.exp(-level)
        cosine, sine = cos_t[...], sin_t[...]
        d_re, d_im = forc[rows, :lanes], forc[rows, lanes:]
        w_re = shrink * (cosine * d_re + sine * d_im)
        w_im = shrink * (cosine * d_im - sine * d_re)
        forc[rows, :lanes] = w_re
        forc[rows, lanes:] = w_im
        grow_buf[rows, :] = grow
        e_re, e_im = grow[last] * cosine[last], grow[last] * sine[last]
        t_re = c_re + jnp.sum(w_re, axis=0, keepdims=True)
        t_im = c_im + jnp.sum(w_im, axis=0, keepdims=True)
        return (
            a_re * e_re - a_im * e_im,
            a_re * e_im + a_im * e_re,
            e_re * t_re - e_im * t_im,
            e_re * t_im + e_im * t_re,
        )

    zero = jnp.zeros((1, lanes), F32)
    ended = lax.fori_loop(0, count // BLOCK, first_pass, (zero + 1.0, zero, zero, zero))
    half = lanes // 2
    for r in range(4):
        summ[r : r + 1, :] = ended[r][:, :half]
        summ[4 + r : 5 + r, :] = ended[r][:, half:]

    def summ_copy(d):
        return remote(summ, summ_in.at[sp], sum_s.at[d], sum_r.at[d], (lax.rem(sp + d, n), tp))

    for d in range(1, n):

        @pl.when(sp + d < n)
        def _():
            summ_copy(d).start()

    ring_send(merge_set, 2) if hops > 2 else None

    @pl.when(sp > 0)
    def _():
        halo_copy.wait_recv()

    ext[0:BLOCK, :] = halo[...].astype(F32)
    reach = taps.shape[0] - 1

    @pl.loop(0, count // tile)
    def _(i):
        start = pl.multiple_of(i * tile, tile)
        window = ext[pl.ds(start, tile + BLOCK), :]
        total = jnp.zeros((tile, width), F32)
        for k in range(reach + 1):
            at = BLOCK - reach + k
            total += taps[k : k + 1, :] * window[at : at + tile, :]
        raw[pl.ds(start, tile), :] = total

    lane = lax.broadcasted_iota(jnp.int32, (count, 128), 1)
    values = raw[...]
    first = jnp.sum(values, axis=1, keepdims=True)
    second = jnp.sum(values * values, axis=1, keepdims=True)
    packed = jnp.where(lane == 0, first, jnp.where(lane == 1, second, 0.0))
    stat[...] = packed.T[0:8, :]

    def stat_copy(d):
        return remote(stat, stat_in.at[d], st_s.at[d], st_r.at[d], (sp, lax.rem(tp + d, ntp)))

    for d in range(1, ntp):
        stat_copy(d).start()
    for step in range(3, hops):
        ring_send(merge_set, step)

    for d in range(1, n):

        @pl.when(sp >= d)
        def _():
            summ_copy(d).wait_recv()

    def unpack(block):
        return [jnp.concatenate([block[r : r + 1], block[4 + r : 5 + r]], axis=1) for r in range(4)]

    h_re, h_im = init[0:1, :], init[1:2, :]
    for q in range(n - 1):
        a_re, a_im, b_re, b_im = unpack(summ_in[q])
        n_re = a_re * h_re - a_im * h_im + b_re
        n_im = a_re * h_im + a_im * h_re + b_im
        h_re = jnp.where(q < sp, n_re, h_re)
        h_im = jnp.where(q < sp, n_im, h_im)

    lower_half = lower.astype(BF16)

    def second_pass(k, state):
        c_re, c_im = state
        rows = pl.ds(pl.multiple_of(k * BLOCK, BLOCK), BLOCK)
        high, low = split(forc[rows, :])
        summed = dot(lower_half, high) + dot(lower_half, low)
        t_re = summed[:, :lanes] + c_re
        t_im = summed[:, lanes:] + c_im
        grow = grow_buf[rows, :]
        g_re, g_im = grow * cos_t[...], grow * sin_t[...]
        x_re = g_re * t_re - g_im * t_im
        x_im = g_re * t_im + g_im * t_re
        xs[rows, :lanes] = x_re.astype(BF16)
        xs[rows, lanes:] = x_im.astype(BF16)
        return x_re[last], x_im[last]

    lax.fori_loop(0, count // BLOCK, second_pass, (h_re, h_im))

    @pl.loop(0, count // big)
    def _(i):
        rows = pl.ds(pl.multiple_of(i * big, big), big)
        total = dot(xs[rows, :], cout[...])
        total += skip[...] * u_buf[rows, :].astype(F32)
        ssm[rows, :] = jax.nn.gelu(total).astype(BF16)

    for d in range(1, ntp):
        stat_copy(d).wait_recv()
    sums = stat[...]
    for d in range(1, ntp):
        sums += stat_in[d]
    channels = width * ntp
    middle_row = sums[0:1] / channels
    inverse_row = lax.rsqrt(sums[1:2] / channels - middle_row * middle_row + epsilon)
    row = lax.broadcasted_iota(jnp.int32, (128, count), 0)
    columns = jnp.where(row == 0, middle_row, inverse_row).T
    scaled = (raw[...] - columns[:, 0:1]) * columns[:, 1:2] * chgain[...]
    conv[...] = jax.nn.silu(scaled).astype(BF16)

    ring_end(merge_set)
    quarters, block_rows = snd.shape[1], snd.shape[2]
    per = n // quarters
    cw = merge_s.shape[1]

    def product(block, q):
        rows = pl.ds(pl.multiple_of(block * block_rows, block_rows), block_rows)
        a, b = ssm[rows, :], conv[rows, :]
        outs = []
        for o in range(q * per, (q + 1) * per):
            outs.append((dot(a, mgat[0, o]) + dot(b, mgat[1, o])).astype(BF16))
        return outs

    def to_partner(d, q):
        return remote(snd.at[d, q], rp.at[d, q], rp_s.at[d, q], rp_r.at[d, q], (sp, partner))

    def across(d, q):
        where = (sp, lax.rem(y + d, ny) * 2 + core)
        return remote(s2.at[d, q], r2.at[d, q], r2_s.at[d, q], r2_r.at[d, q], where)

    order = list(range(1, ny)) + [0]

    def fill(buffer, d, q, which):
        for i, value in enumerate(product(lax.rem(y + d, ny) * 2 + which, q)):
            buffer[d, q, :, i * cw : (i + 1) * cw] = value

    def relay(d, q):
        to_partner(d, q).wait_recv()
        s2[d, q] = (own[d, q].astype(F32) + rp[d, q].astype(F32)).astype(BF16)
        across(d, q).start()

    for d in order:
        for q in range(quarters):
            fill(snd, d, q, 1 - core)
            to_partner(d, q).start()
            fill(own, d, q, core)
            if d and q:
                relay(d, q - 1)
        if d:
            relay(d, quarters - 1)
    for q in range(quarters):
        to_partner(0, q).wait_recv()
        total = own[0, q].astype(F32) + rp[0, q].astype(F32)
        for d in range(1, ny):
            across(d, q).wait_recv()
            total += r2[d, q].astype(F32)
        out[:, q * per * cw : (q + 1) * per * cw] = total.astype(BF16)

    for w in range(5):
        for side in range(2):
            for step in range(hops):
                piece(w, side, step).wait_send()
    for d in range(ny):
        tok_copy(d).wait_send()
        if d:
            tok_forward(d).wait_send()
        for q in range(quarters):
            to_partner(d, q).wait_send()
            if d:
                across(d, q).wait_send()
    for d in range(1, ntp):
        stat_copy(d).wait_send()

    @pl.when(sp < n - 1)
    def _():
        halo_copy.wait_send()

    for d in range(1, n):

        @pl.when(sp + d < n)
        def _():
            summ_copy(d).wait_send()


def fused(
    n, ntp, tokens, norm_gain, proj_state, proj_value, proj_gate, eigen_real, eigen_imag,
    log_step, decay_shift, state_input, state_readout_matrices, skip_gain, init_state,
    conv_taps, channel_gain, merge_state, merge_conv,
):
    count, part = tokens.shape
    groups, states = eigen_real.shape
    width = proj_state.shape[1]
    lanes = groups * states
    features = part * ntp
    step = jnp.exp(log_step)
    base = (eigen_real * step[:, None]).reshape(1, lanes)
    theta = (eigen_imag * step[:, None]).reshape(1, lanes)
    counts = (jnp.arange(BLOCK) + 1).astype(F32)[:, None]
    angle = counts * theta
    b_re, b_im = input_matrix(eigen_real, eigen_imag, step, state_input)
    group = width // groups
    same = jnp.arange(width)[:, None] // group == jnp.arange(lanes)[None, :] // states

    def spread_out(matrix):
        tiled = jnp.tile(matrix.reshape(width, states), (1, groups))
        return jnp.where(same, tiled, 0.0)

    binp = jnp.concatenate([spread_out(b_re), spread_out(b_im)], axis=1)
    cout = jnp.concatenate(
        [spread_out(state_readout_matrices[0]), -spread_out(state_readout_matrices[1])], axis=1
    ).astype(BF16).T
    expand = (jnp.arange(groups)[:, None] == jnp.arange(lanes)[None, :] // states).astype(F32)
    quarters = min(4, n)
    ny = ntp // 2
    block_rows = count // ntp
    cw = merge_state.shape[1] * n // quarters
    pieces = pltpu.VMEM((ny, quarters, block_rows, cw), BF16)
    vmem = pl.BlockSpec(memory_space=pltpu.VMEM)
    hops = n // 2
    dma = pltpu.SemaphoreType.DMA
    return pl.pallas_call(
        functools.partial(mixer_kernel, n, ntp),
        out_shape=jax.ShapeDtypeStruct((block_rows, features), BF16),
        in_specs=[vmem] * 18,
        out_specs=vmem,
        scratch_shapes=[
            pltpu.VMEM((ntp, count, part), BF16),
            pltpu.VMEM((count, features), BF16),
            pltpu.VMEM((3, n) + proj_state.shape, BF16),
            pltpu.VMEM((2, n) + merge_state.shape, BF16),
            pltpu.VMEM((count, width), BF16),
            pltpu.VMEM((count, 2 * lanes), F32),
            pltpu.VMEM((count, lanes), F32),
            pltpu.VMEM((count, 2 * lanes), BF16),
            pltpu.VMEM((count + BLOCK, width), F32),
            pltpu.VMEM((count, width), F32),
            pltpu.VMEM((count, width), BF16),
            pltpu.VMEM((count, width), BF16),
            pltpu.VMEM((BLOCK, width), BF16),
            pltpu.VMEM((BLOCK, width), BF16),
            pltpu.VMEM((8, lanes // 2), F32),
            pltpu.VMEM((n, 8, lanes // 2), F32),
            pltpu.VMEM((8, count), F32),
            pltpu.VMEM((ntp, 8, count), F32),
            pieces, pieces, pieces, pieces, pieces,
            dma((6,)), dma((ny,)), dma((ny,)), dma((ny,)), dma((ny,)),
            dma((5, 2, hops)), dma((5, 2, hops)), dma, dma,
            dma((n,)), dma((n,)), dma((ntp,)), dma((ntp,)),
            dma((ny, quarters)), dma((ny, quarters)), dma((ny, quarters)), dma((ny, quarters)),
        ],
        compiler_params=pltpu.CompilerParams(
            collective_id=0, has_side_effects=True, vmem_limit_bytes=60 * 1024 * 1024
        ),
        name="mixer",
    )(
        tokens, norm_gain.reshape(1, features), proj_state, proj_value, proj_gate,
        decay_shift.T, expand, counts * base, jnp.cos(angle), jnp.sin(angle), binp, cout,
        skip_gain.reshape(1, width), init_state.reshape(2, lanes), conv_taps,
        channel_gain.reshape(1, width), merge_state, merge_conv,
    )


def per_device_any(n, ntp, *args):
    tokens, merge_state = args[0], args[15]
    fits = (
        n % 8 == 0 and ntp % 2 == 0 and args[2].shape[0] % 128 == 0 and merge_state.shape[1] % 128 == 0
        and tokens.shape[0] % 128 == 0 and args[5].size % 256 == 0 and args[13].shape[0] <= BLOCK
    )
    if fits:
        return fused(n, ntp, *args)
    return per_device(*args)


def solution(mesh):
    return jax.shard_map(
        functools.partial(per_device_any, mesh.shape["sp"], mesh.shape["tp"]),
        mesh=mesh,
        in_specs=(
            P("sp", "tp"),
            P(),
            P("sp", "tp"),
            P("sp", "tp"),
            P("sp", "tp"),
            P("tp", None),
            P("tp", None),
            P("tp"),
            P("tp", "sp"),
            P(None, "tp", None, None),
            P(None, "tp", None, None),
            P("tp"),
            P(None, "tp", None),
            P(None, "tp"),
            P("tp"),
            P("tp", "sp"),
            P("tp", "sp"),
        ),
        out_specs=P(("sp", "tp"), None),
        check_vma=False,
    )
```

```python
import functools

import jax
import jax.numpy as jnp
from jax import lax
from jax.experimental import pallas as pl
from jax.experimental.pallas import tpu as pltpu
from jax.sharding import PartitionSpec as P

CONV_W = 1024


epsilon = 1e-06
exact_precision = lax.Precision.HIGHEST


def entering(value, axis, join, neutral):
    count, mine = (lax.axis_size(axis), lax.axis_index(axis))
    pieces = jax.tree.map(lambda part: lax.all_gather(part, axis), value)
    total = jax.tree.map(
        lambda part, zero: jnp.full_like(part, 0) + jnp.asarray(zero, part.dtype), value, neutral
    )

    def hop(position, total):
        longer = join(total, jax.tree.map(lambda part: part[position], pieces))
        return jax.tree.map(lambda new, old: jnp.where(position < mine, new, old), longer, total)

    return lax.fori_loop(0, count - 1, hop, total)


def passed_along(block, axis, distance):
    devices = range(lax.axis_size(axis))
    route = [(i - distance, i) for i in devices if i - distance in devices]
    return lax.ppermute(block, axis, route)


def round_half(value):
    return lax.optimization_barrier(value.astype(jnp.bfloat16))


def input_matrix(eigen_real, eigen_imag, step, state_input):
    base = eigen_real * step[:, None]
    theta = eigen_imag * step[:, None]
    magnitude = jnp.exp(base)
    near_re = magnitude * jnp.cos(theta) - 1.0
    near_im = magnitude * jnp.sin(theta)
    modulus = eigen_real * eigen_real + eigen_imag * eigen_imag
    ratio_re = (near_re * eigen_real + near_im * eigen_imag) / modulus
    ratio_im = (near_im * eigen_real - near_re * eigen_imag) / modulus
    in_re = state_input[0]
    in_im = state_input[1]
    discrete_decay_real = ratio_re[:, None, :] * in_re - ratio_im[:, None, :] * in_im
    discrete_decay_imaginary = ratio_re[:, None, :] * in_im + ratio_im[:, None, :] * in_re
    return (discrete_decay_real, discrete_decay_imaginary)


def block_states(c_re, c_im, delta_real, delta_imaginary, shift, base, theta, counts, lower):
    level = jnp.cumsum(shift, axis=0)[:, :, None] + counts * base
    angle = counts * theta
    cosine = jnp.cos(angle)
    sine = jnp.sin(angle)
    grow = jnp.exp(level)
    shrink = jnp.exp(-level)
    w_re = shrink * (cosine * delta_real + sine * delta_imaginary)
    w_im = shrink * (cosine * delta_imaginary - sine * delta_real)
    length, groups, states = delta_real.shape
    stacked = jnp.concatenate([w_re, w_im], axis=1).reshape(length, 2 * groups * states)
    summed = jnp.dot(lower, stacked, precision=exact_precision).reshape(length, 2 * groups, states)
    t_re = summed[:, :groups] + c_re
    t_im = summed[:, groups:] + c_im
    input_real = grow * (cosine * t_re - sine * t_im)
    input_imaginary = grow * (cosine * t_im + sine * t_re)
    return (input_real, input_imaginary)


def chain(earlier, later):
    a_re, a_im, b_re, b_im = earlier
    c_re, c_im, delta_real, delta_imaginary = later
    return (
        a_re * c_re - a_im * c_im,
        a_re * c_im + a_im * c_re,
        c_re * b_re - c_im * b_im + delta_real,
        c_re * b_im + c_im * b_re + delta_imaginary,
    )


def state_local(
    u_in, eigen_real, eigen_imag, log_step, decay_shift, state_input, state_readout_matrices
):
    count, width = u_in.shape
    groups, states = eigen_real.shape
    group = width // groups
    step = jnp.exp(log_step)
    base = eigen_real * step[:, None]
    theta = eigen_imag * step[:, None]
    discrete_decay_real, discrete_decay_imaginary = input_matrix(
        eigen_real, eigen_imag, step, state_input
    )
    float_values = u_in.astype(jnp.float32).reshape(count, groups, group)
    forcing_real = jnp.einsum(
        "ovi,viu->ovu", float_values, discrete_decay_real, precision=exact_precision
    )
    forcing_imaginary = jnp.einsum(
        "ovi,viu->ovu", float_values, discrete_decay_imaginary, precision=exact_precision
    )
    shift = decay_shift.T
    length = min(32, count)
    blocks = count // length
    counts = (jnp.arange(length) + 1).astype(jnp.float32)[:, None, None]
    lower = (jnp.arange(length)[:, None] >= jnp.arange(length)[None, :]).astype(jnp.float32)

    def advance(carry, inputs):
        delta_real, delta_imaginary, block_shift = inputs
        input_real, input_imaginary = block_states(
            carry[0], carry[1], delta_real, delta_imaginary, block_shift, base, theta, counts, lower
        )
        return ((input_real[-1], input_imaginary[-1]), (input_real, input_imaginary))

    zero = jnp.zeros((groups, states), jnp.float32)
    last, (input_real, input_imaginary) = lax.scan(
        advance,
        (zero, zero),
        (
            forcing_real.reshape(blocks, length, groups, states),
            forcing_imaginary.reshape(blocks, length, groups, states),
            shift.reshape(blocks, length, groups),
        ),
    )
    input_real = input_real.reshape(count, groups, states)
    input_imaginary = input_imaginary.reshape(count, groups, states)
    local_output = jnp.einsum(
        "lan,arn->lar", input_real, state_readout_matrices[0], precision=exact_precision
    ) - jnp.einsum(
        "lan,arn->lar", input_imaginary, state_readout_matrices[1], precision=exact_precision
    )
    whole_count = (jnp.arange(count) + 1).astype(jnp.float32)[:, None, None]
    level = jnp.cumsum(shift, axis=0)[:, :, None] + whole_count * base
    angle = whole_count * theta
    grow = jnp.exp(level)
    exponent_real = grow * jnp.cos(angle)
    exponent_imaginary = grow * jnp.sin(angle)
    summary = (exponent_real[-1], exponent_imaginary[-1], last[0], last[1])
    return (local_output, exponent_real, exponent_imaginary, summary)


def carry_in(summary, init_state):
    groups, states = summary[0].shape
    ones = jnp.ones((groups, states), jnp.float32)
    zeros = jnp.zeros((groups, states), jnp.float32)
    identity = (ones, zeros, zeros, zeros)
    before = entering(summary, "sp", chain, identity)
    a_re, a_im, b_re, b_im = before
    s_re = init_state[0]
    s_im = init_state[1]
    return (a_re * s_re - a_im * s_im + b_re, a_re * s_im + a_im * s_re + b_im)


def state_finish(
    local_output,
    exponent_real,
    exponent_imaginary,
    carried,
    state_readout_matrices,
    skip_gain,
    u_in,
):
    h_re, h_im = carried
    output_real = state_readout_matrices[0]
    output_imaginary = state_readout_matrices[1]
    blend_real = output_real * h_re[:, None, :] - output_imaginary * h_im[:, None, :]
    blend_imaginary = output_real * h_im[:, None, :] + output_imaginary * h_re[:, None, :]
    total = (
        local_output
        + jnp.einsum("lan,arn->lar", exponent_real, blend_real, precision=exact_precision)
        - jnp.einsum("lan,arn->lar", exponent_imaginary, blend_imaginary, precision=exact_precision)
    )
    count, width = u_in.shape
    groups = local_output.shape[1]
    float_values = u_in.astype(jnp.float32).reshape(count, groups, width // groups)
    total = total + skip_gain.reshape(groups, width // groups) * float_values
    return jax.nn.gelu(total).reshape(count, width).astype(jnp.bfloat16)


def conv_branch(value, gate, conv_taps, channel_gain):
    glu = round_half(value.astype(jnp.float32) * jax.nn.sigmoid(gate.astype(jnp.float32)))
    reach = conv_taps.shape[0] - 1
    count = glu.shape[0]
    before = passed_along(glu[count - reach :], "sp", 1)
    extended = jnp.concatenate([before, glu], axis=0).astype(jnp.float32)
    raw = jnp.zeros(glu.shape, jnp.float32)
    for offset in range(reach + 1):
        raw = raw + conv_taps[offset] * extended[offset : offset + count]
    first, second = lax.psum(
        (jnp.sum(raw, axis=1, keepdims=True), jnp.sum(raw * raw, axis=1, keepdims=True)), "tp"
    )
    middle = first / CONV_W
    spread = second / CONV_W - middle * middle
    scaled = (raw - middle) * lax.rsqrt(spread + epsilon) * channel_gain
    return jax.nn.silu(scaled).astype(jnp.bfloat16)


def per_device(
    tokens,
    norm_gain,
    proj_state,
    proj_value,
    proj_gate,
    eigen_real,
    eigen_imag,
    log_step,
    decay_shift,
    state_input,
    state_readout_matrices,
    skip_gain,
    init_state,
    conv_taps,
    channel_gain,
    merge_state,
    merge_conv,
):
    whole = lax.all_gather(tokens, "tp", axis=1, tiled=True)
    wide = whole.astype(jnp.float32)
    normed = (
        wide * lax.rsqrt(jnp.mean(wide * wide, axis=1, keepdims=True) + epsilon) * norm_gain
    ).astype(jnp.bfloat16)
    pieces = (
        lax.all_gather(proj_state, "sp", axis=0, tiled=True),
        lax.all_gather(proj_value, "sp", axis=0, tiled=True),
        lax.all_gather(proj_gate, "sp", axis=0, tiled=True),
    )
    state_sum, value_sum, gate_sum = tuple(
        (jnp.dot(normed, piece, preferred_element_type=jnp.float32) for piece in pieces)
    )
    u_in = round_half(state_sum)
    local_output, exponent_real, exponent_imaginary, summary = state_local(
        u_in, eigen_real, eigen_imag, log_step, decay_shift, state_input, state_readout_matrices
    )
    carried = carry_in(summary, init_state)
    conv_out = conv_branch(round_half(value_sum), round_half(gate_sum), conv_taps, channel_gain)
    ssm_out = state_finish(
        local_output,
        exponent_real,
        exponent_imaginary,
        carried,
        state_readout_matrices,
        skip_gain,
        u_in,
    )
    full_state, full_conv = (
        lax.all_gather(merge_state, "sp", axis=1, tiled=True),
        lax.all_gather(merge_conv, "sp", axis=1, tiled=True),
    )
    return lax.psum_scatter(
        (
            jnp.dot(ssm_out, full_state, preferred_element_type=jnp.float32)
            + jnp.dot(conv_out, full_conv, preferred_element_type=jnp.float32)
        ).astype(jnp.bfloat16),
        "tp",
        scatter_dimension=0,
        tiled=True,
    )


MESH = pl.DeviceIdType.MESH
F32 = jnp.float32
BF16 = jnp.bfloat16
BLOCK = 32


def dot(a, b):
    return jnp.dot(a, b, preferred_element_type=F32)


def dot_exact(a, b):
    return jnp.dot(a, b, preferred_element_type=F32, precision=exact_precision)


def split(value):
    high = value.astype(BF16)
    return high, (value - high.astype(F32)).astype(BF16)


def ring_position(index, n):
    return jnp.where(index % 2 == 0, index // 2, n - 1 - index // 2)


def ring_index(position, n):
    position = lax.rem(position + 2 * n, n)
    return jnp.where(position < n // 2, 2 * position, 2 * (n - 1 - position) + 1)


def mixer_kernel(
    n, ntp,
    tokens, gain, proj_s, proj_v, proj_g, eig_re, eig_im, log_step, decay,
    state_in, state_out, skip, init, taps, chgain, merge_s, merge_c,
    out,
    shift, base_t, cos_t, sin_t, bin_high, bin_low, cout, into_re, into_im, back_re, back_im, held,
    tok, normed, gat, mgat, u_buf, forc, xs, ext, raw, ssm, conv,
    halo, glu_tail, summ, summ_in, stat, stat_in, snd, own, rp, s2, r2,
    loc_sem, tok_s, tok_r, fwd_s, fwd_r, ring_s, ring_r, halo_s, halo_r,
    sum_s, sum_r, st_s, st_r, rp_s, rp_r, r2_s, r2_r,
):
    sp = lax.axis_index("sp")
    tp = lax.axis_index("tp")
    ny = ntp // 2
    y, core = tp // 2, tp % 2
    partner = y * 2 + 1 - core
    pos = ring_position(sp, n)
    right, left = ring_index(pos + 1, n), ring_index(pos - 1, n)
    count, width = u_buf.shape
    groups, states = eig_re.shape
    lanes = groups * states
    part = tokens.shape[1]
    rows_w = proj_s.shape[0]

    halo[...] = jnp.zeros_like(halo)
    summ_in[...] = jnp.zeros_like(summ_in)

    barrier = pltpu.get_barrier_semaphore()
    for d in range(1, n):
        pl.semaphore_signal(barrier, inc=1, device_id=(lax.rem(sp + d, n), tp), device_id_type=MESH)
    for d in range(1, ntp):
        pl.semaphore_signal(barrier, inc=1, device_id=(sp, lax.rem(tp + d, ntp)), device_id_type=MESH)
    pl.semaphore_wait(barrier, n + ntp - 2)

    def remote(src, dst, s, r, where):
        return pltpu.make_async_remote_copy(
            src_ref=src, dst_ref=dst, send_sem=s, recv_sem=r, device_id=where, device_id_type=MESH
        )

    sources = (proj_s, proj_v, proj_g, merge_s, merge_c)
    hops = n // 2

    def slot(w, origin):
        return gat.at[w, origin] if w < 3 else mgat.at[w - 3, origin]

    def piece(w, side, step):
        origin = ring_index(pos - step if side == 0 else pos + step, n)
        where = (right if side == 0 else left, tp)
        src = sources[w] if step == 0 else slot(w, origin)
        dst = slot(w, origin)
        if step == hops - 1:
            half = src.shape[0] // 2
            window = pl.ds(side * half, half)
            src, dst = src.at[window], dst.at[window]
        return remote(src, dst, ring_s.at[w, side, step], ring_r.at[w, side, step], where)

    def ring_send(ws, step):
        for w in ws:
            for side in range(2):
                if step > 0:
                    piece(w, side, step - 1).wait_recv()
                piece(w, side, step).start()

    def ring_end(ws):
        for w in ws:
            for side in range(2):
                piece(w, side, hops - 1).wait_recv()

    ring_send([0, 1], 0)

    def tok_copy(d):
        where = (sp, lax.rem(y + d, ny) * 2 + core) if d else (sp, partner)
        return remote(tokens, tok.at[tp], tok_s.at[d], tok_r.at[d], where)

    def tok_forward(d):
        origin = lax.rem(y - d + ny, ny) * 2 + core
        return remote(tok.at[origin], tok.at[origin], fwd_s.at[d], fwd_r.at[d], (sp, partner))

    for d in list(range(1, ny)) + [0]:
        tok_copy(d).start()
    local = [pltpu.make_async_copy(tokens, tok.at[tp], loc_sem.at[5])]
    for w in range(5):
        local.append(pltpu.make_async_copy(sources[w], slot(w, sp), loc_sem.at[w]))
    for c in local:
        c.start()

    row_i = lax.broadcasted_iota(jnp.int32, (BLOCK, BLOCK), 0)
    col_i = lax.broadcasted_iota(jnp.int32, (BLOCK, BLOCK), 1)
    lower = (row_i >= col_i).astype(F32)
    last = slice(BLOCK - 1, BLOCK)

    def lane_of(rows):
        return lax.broadcasted_iota(jnp.int32, (rows, lanes), 1)

    def row_of(rows):
        return lax.broadcasted_iota(jnp.int32, (rows, lanes), 0)

    repeat = (lax.rem(lane_of(states), states) == row_of(states)).astype(F32)
    mine = lax.div(lane_of(groups), states) == row_of(groups)
    expand = mine.astype(F32)

    def to_row(matrix):
        return jnp.sum(jnp.where(mine, dot_exact(matrix, repeat), 0.0), axis=0, keepdims=True)

    square_row = lax.broadcasted_iota(jnp.int32, (groups, groups), 0)
    square_col = lax.broadcasted_iota(jnp.int32, (groups, groups), 1)
    steps = jnp.broadcast_to(jnp.exp(log_step[...]), (groups, groups))
    step_size = jnp.sum(jnp.where(square_row == square_col, steps, 0.0), axis=1, keepdims=True)
    real_row, imag_row = to_row(eig_re[...]), to_row(eig_im[...])
    base_row = to_row(eig_re[...] * step_size)
    theta_row = to_row(eig_im[...] * step_size)
    counts = (row_of(BLOCK) + 1).astype(F32)
    base_t[...] = counts * base_row
    cos_t[...] = jnp.cos(counts * theta_row)
    sin_t[...] = jnp.sin(counts * theta_row)
    magnitude = jnp.exp(base_row)
    near_re = magnitude * cos_t[0:1, :] - 1.0
    near_im = magnitude * sin_t[0:1, :]
    modulus = real_row * real_row + imag_row * imag_row
    ratio_re = (near_re * real_row + near_im * imag_row) / modulus
    ratio_im = (near_im * real_row - near_re * imag_row) / modulus
    group = width // groups
    chunk = 256
    for j in range(lanes // chunk):
        cols = slice(j * chunk, (j + 1) * chunk)
        later = slice(lanes + j * chunk, lanes + (j + 1) * chunk)
        spot = lax.broadcasted_iota(jnp.int32, (width, chunk), 1) + j * chunk
        whose = lax.div(lax.broadcasted_iota(jnp.int32, (width, chunk), 0), group)
        same = lax.div(spot, states) == whose
        m_re = dot_exact(state_in[0:width, :], repeat[:, cols])
        m_im = dot_exact(state_in[width : 2 * width, :], repeat[:, cols])
        r_re, r_im = ratio_re[:, cols], ratio_im[:, cols]
        bin_high[:, cols], bin_low[:, cols] = split(jnp.where(same, r_re * m_re - r_im * m_im, 0.0))
        bin_high[:, later], bin_low[:, later] = split(jnp.where(same, r_re * m_im + r_im * m_re, 0.0))
        m_re = dot_exact(state_out[0:width, :], repeat[:, cols])
        m_im = dot_exact(state_out[width : 2 * width, :], repeat[:, cols])
        cout[:, cols] = jnp.where(same, m_re, 0.0).astype(BF16)
        cout[:, later] = jnp.where(same, -m_im, 0.0).astype(BF16)
    start_re, start_im = to_row(init[0:groups, :]), to_row(init[groups : 2 * groups, :])
    fill_rows = jnp.zeros((128 - groups, count), F32)
    shift[...] = jnp.concatenate([decay[...], fill_rows], axis=0).T

    ring_send([0, 1], 1)

    def prepare(k, state):
        a_re, a_im = state
        rows = pl.ds(pl.multiple_of(k * BLOCK, BLOCK), BLOCK)
        level = dot_exact(dot_exact(lower, shift[rows, :])[:, :groups], expand) + base_t[...]
        grow, shrink = jnp.exp(level), jnp.exp(-level)
        cosine, sine = cos_t[...], sin_t[...]
        into_re[rows, :] = shrink * cosine
        into_im[rows, :] = shrink * sine
        g_re, g_im = grow * cosine, grow * sine
        back_re[rows, :] = g_re
        back_im[rows, :] = g_im
        held[0, pl.ds(k, 1), :] = a_re
        held[1, pl.ds(k, 1), :] = a_im
        e_re, e_im = g_re[last], g_im[last]
        return a_re * e_re - a_im * e_im, a_re * e_im + a_im * e_re

    zero = jnp.zeros((1, lanes), F32)
    blocks = count // BLOCK
    decayed = lax.fori_loop(0, blocks // 2, prepare, (zero + 1.0, zero))
    ring_send([0, 1], 2)
    for d in range(1, ny):
        tok_copy(d).wait_recv()
        tok_forward(d).start()
    decayed = lax.fori_loop(blocks // 2, blocks, prepare, decayed)
    for step in range(3, hops - 1):
        ring_send([0, 1], step)
    ring_send([0], hops - 1)
    ring_send([2], 0)
    ring_send([1], hops - 1)
    tok_copy(0).wait_recv()
    for c in local:
        c.wait()
    for d in range(1, ny):
        tok_forward(d).wait_recv()

    tile = 64

    @pl.loop(0, count // tile)
    def _(i):
        rows = pl.ds(pl.multiple_of(i * tile, tile), tile)
        pieces = [tok[j, rows, :].astype(F32) for j in range(ntp)]
        square = sum(jnp.sum(p * p, axis=1, keepdims=True) for p in pieces)
        scale = lax.rsqrt(square / (part * ntp) + epsilon)
        for j in range(ntp):
            cols = slice(j * part, (j + 1) * part)
            normed[rows, cols] = (pieces[j] * scale * gain[:, cols]).astype(BF16)

    ring_end([0])

    big = 128

    def project(w, i):
        rows = pl.ds(pl.multiple_of(i * big, big), big)
        total = dot(normed[rows, 0:rows_w], gat[w, 0])
        for o in range(1, n):
            total += dot(normed[rows, o * rows_w : (o + 1) * rows_w], gat[w, o])
        return rows, total.astype(BF16)

    @pl.loop(0, count // big)
    def _(i):
        rows, u = project(0, i)
        u_buf[rows, :] = u

    wide = 256

    @pl.loop(0, 2 * lanes // wide)
    def _(j):
        cols = pl.ds(pl.multiple_of(j * wide, wide), wide)
        forc[:, cols] = dot(u_buf[...], bin_high[:, cols]) + dot(u_buf[...], bin_low[:, cols])

    ring_send([3], 0)
    ring_send([2], 1)

    def first_pass(k, state):
        c_re, c_im = state
        rows = pl.ds(pl.multiple_of(k * BLOCK, BLOCK), BLOCK)
        held[2, pl.ds(k, 1), :] = c_re
        held[3, pl.ds(k, 1), :] = c_im
        d_re, d_im = forc[rows, :lanes], forc[rows, lanes:]
        w_re = into_re[rows, :] * d_re + into_im[rows, :] * d_im
        w_im = into_re[rows, :] * d_im - into_im[rows, :] * d_re
        forc[rows, :lanes] = w_re
        forc[rows, lanes:] = w_im
        final = pl.ds(k * BLOCK + BLOCK - 1, 1)
        e_re, e_im = back_re[final, :], back_im[final, :]
        t_re = c_re + jnp.sum(w_re, axis=0, keepdims=True)
        t_im = c_im + jnp.sum(w_im, axis=0, keepdims=True)
        return e_re * t_re - e_im * t_im, e_re * t_im + e_im * t_re

    ended = decayed + lax.fori_loop(0, blocks, first_pass, (zero, zero))
    half = lanes // 2
    for r in range(4):
        summ[r : r + 1, :] = ended[r][:, :half]
        summ[4 + r : 5 + r, :] = ended[r][:, half:]

    def summ_copy(d):
        return remote(summ, summ_in.at[sp], sum_s.at[d], sum_r.at[d], (lax.rem(sp + d, n), tp))

    for d in range(1, n):

        @pl.when(sp + d < n)
        def _():
            summ_copy(d).start()

    ring_send([4], 0)
    ring_send([2], 2)


    for d in range(1, n):

        @pl.when(sp >= d)
        def _():
            summ_copy(d).wait_recv()

    def unpack(block):
        return [jnp.concatenate([block[r : r + 1], block[4 + r : 5 + r]], axis=1) for r in range(4)]

    h_re, h_im = start_re, start_im
    for q in range(n - 1):
        a_re, a_im, b_re, b_im = unpack(summ_in[q])
        n_re = a_re * h_re - a_im * h_im + b_re
        n_im = a_re * h_im + a_im * h_re + b_im
        h_re = jnp.where(q < sp, n_re, h_re)
        h_im = jnp.where(q < sp, n_im, h_im)

    lower_half = lower.astype(BF16)

    def second_pass(k, _):
        rows = pl.ds(pl.multiple_of(k * BLOCK, BLOCK), BLOCK)
        one = pl.ds(k, 1)
        a_re, a_im = held[0, one, :], held[1, one, :]
        c_re = held[2, one, :] + a_re * h_re - a_im * h_im
        c_im = held[3, one, :] + a_re * h_im + a_im * h_re
        high, low = split(forc[rows, :])
        summed = dot(lower_half, high) + dot(lower_half, low)
        t_re = summed[:, :lanes] + c_re
        t_im = summed[:, lanes:] + c_im
        g_re, g_im = back_re[rows, :], back_im[rows, :]
        xs[rows, :lanes] = (g_re * t_re - g_im * t_im).astype(BF16)
        xs[rows, lanes:] = (g_re * t_im + g_im * t_re).astype(BF16)
        return 0

    lax.fori_loop(0, blocks, second_pass, 0)
    ring_send([3], 1)
    for step in range(3, hops - 1):
        ring_send([2], step)
    ring_send([2], hops - 1)
    ring_send([4], 1)
    for step in range(2, hops - 2):
        ring_send([3, 4], step)
    ring_end([1, 2])

    @pl.loop(0, count // big)
    def _(i):
        rows, value = project(1, i)
        rows, gate = project(2, i)
        glu = (value.astype(F32) * jax.nn.sigmoid(gate.astype(F32))).astype(BF16)
        ext[pl.ds(pl.multiple_of(BLOCK + i * big, BLOCK), big), :] = glu.astype(F32)

    glu_tail[...] = ext[count : count + BLOCK, :].astype(BF16)
    halo_to = lax.rem(sp + 1, n)
    halo_copy = remote(glu_tail, halo, halo_s, halo_r, (halo_to, tp))

    @pl.when(sp < n - 1)
    def _():
        halo_copy.start()

    reach = taps.shape[0] - 1
    ring_send([3, 4], hops - 2)

    def taps_on(start):
        window = ext[pl.ds(start, tile + BLOCK), :]
        total = jnp.zeros((tile, width), F32)
        for k in range(reach + 1):
            at = BLOCK - reach + k
            total += taps[k : k + 1, :] * window[at : at + tile, :]
        raw[pl.ds(start, tile), :] = total

    @pl.loop(1, count // tile)
    def _(i):
        taps_on(pl.multiple_of(i * tile, tile))

    @pl.when(sp > 0)
    def _():
        halo_copy.wait_recv()

    ext[0:BLOCK, :] = halo[...].astype(F32)
    taps_on(0)

    lane = lax.broadcasted_iota(jnp.int32, (count, 128), 1)
    values = raw[...]
    first = jnp.sum(values, axis=1, keepdims=True)
    second = jnp.sum(values * values, axis=1, keepdims=True)
    packed = jnp.where(lane == 0, first, jnp.where(lane == 1, second, 0.0))
    stat[...] = packed.T[0:8, :]

    def stat_copy(d):
        return remote(stat, stat_in.at[d], st_s.at[d], st_r.at[d], (sp, lax.rem(tp + d, ntp)))

    for d in range(1, ntp):
        stat_copy(d).start()
    ring_send([3, 4], hops - 1)

    @pl.loop(0, count // big)
    def _(i):
        rows = pl.ds(pl.multiple_of(i * big, big), big)
        total = lax.dot_general(
            xs[rows, :], cout[...], (((1,), (1,)), ((), ())), preferred_element_type=F32
        )
        total += skip[...] * u_buf[rows, :].astype(F32)
        ssm[rows, :] = jax.nn.gelu(total).astype(BF16)

    for d in range(1, ntp):
        stat_copy(d).wait_recv()
    sums = stat[...]
    for d in range(1, ntp):
        sums += stat_in[d]
    channels = width * ntp
    middle_row = sums[0:1] / channels
    inverse_row = lax.rsqrt(sums[1:2] / channels - middle_row * middle_row + epsilon)
    row = lax.broadcasted_iota(jnp.int32, (128, count), 0)
    columns = jnp.where(row == 0, middle_row, inverse_row).T
    scaled = (raw[...] - columns[:, 0:1]) * columns[:, 1:2] * chgain[...]
    conv[...] = jax.nn.silu(scaled).astype(BF16)

    ring_end([3, 4])
    quarters, block_rows = snd.shape[1], snd.shape[2]
    per = n // quarters
    cw = merge_s.shape[1]

    def product(block, q):
        rows = pl.ds(pl.multiple_of(block * block_rows, block_rows), block_rows)
        a, b = ssm[rows, :], conv[rows, :]
        outs = []
        for o in range(q * per, (q + 1) * per):
            outs.append((dot(a, mgat[0, o]) + dot(b, mgat[1, o])).astype(BF16))
        return outs

    def to_partner(d, q):
        return remote(snd.at[d, q], rp.at[d, q], rp_s.at[d, q], rp_r.at[d, q], (sp, partner))

    def across(d, q):
        where = (sp, lax.rem(y + d, ny) * 2 + core)
        return remote(s2.at[d, q], r2.at[d, q], r2_s.at[d, q], r2_r.at[d, q], where)

    order = list(range(1, ny)) + [0]

    def fill(buffer, d, q, which):
        for i, value in enumerate(product(lax.rem(y + d, ny) * 2 + which, q)):
            buffer[d, q, :, i * cw : (i + 1) * cw] = value

    def relay(d, q):
        to_partner(d, q).wait_recv()
        s2[d, q] = (own[d, q].astype(F32) + rp[d, q].astype(F32)).astype(BF16)
        across(d, q).start()

    for d in order:
        for q in range(quarters):
            fill(snd, d, q, 1 - core)
            to_partner(d, q).start()
            fill(own, d, q, core)
            if d and q:
                relay(d, q - 1)
        if d:
            relay(d, quarters - 1)
    for q in range(quarters):
        to_partner(0, q).wait_recv()
        total = own[0, q].astype(F32) + rp[0, q].astype(F32)
        for d in range(1, ny):
            across(d, q).wait_recv()
            total += r2[d, q].astype(F32)
        out[:, q * per * cw : (q + 1) * per * cw] = total.astype(BF16)

    for w in range(5):
        for side in range(2):
            for step in range(hops):
                piece(w, side, step).wait_send()
    for d in range(ny):
        tok_copy(d).wait_send()
        if d:
            tok_forward(d).wait_send()
        for q in range(quarters):
            to_partner(d, q).wait_send()
            if d:
                across(d, q).wait_send()
    for d in range(1, ntp):
        stat_copy(d).wait_send()

    @pl.when(sp < n - 1)
    def _():
        halo_copy.wait_send()

    for d in range(1, n):

        @pl.when(sp + d < n)
        def _():
            summ_copy(d).wait_send()


def fused(
    n, ntp, tokens, norm_gain, proj_state, proj_value, proj_gate, eigen_real, eigen_imag,
    log_step, decay_shift, state_input, state_readout_matrices, skip_gain, init_state,
    conv_taps, channel_gain, merge_state, merge_conv,
):
    count, part = tokens.shape
    groups, states = eigen_real.shape
    width = proj_state.shape[1]
    lanes = groups * states
    features = part * ntp
    quarters = min(4, n)
    ny = ntp // 2
    block_rows = count // ntp
    cw = merge_state.shape[1] * n // quarters
    pieces = pltpu.VMEM((ny, quarters, block_rows, cw), BF16)
    vmem = pl.BlockSpec(memory_space=pltpu.VMEM)
    hops = n // 2
    dma = pltpu.SemaphoreType.DMA
    return pl.pallas_call(
        functools.partial(mixer_kernel, n, ntp),
        out_shape=jax.ShapeDtypeStruct((block_rows, features), BF16),
        in_specs=[vmem] * 17,
        out_specs=vmem,
        scratch_shapes=[
            pltpu.VMEM((count, 128), F32),
            pltpu.VMEM((BLOCK, lanes), F32),
            pltpu.VMEM((BLOCK, lanes), F32),
            pltpu.VMEM((BLOCK, lanes), F32),
            pltpu.VMEM((width, 2 * lanes), BF16),
            pltpu.VMEM((width, 2 * lanes), BF16),
            pltpu.VMEM((width, 2 * lanes), BF16),
            pltpu.VMEM((count, lanes), F32),
            pltpu.VMEM((count, lanes), F32),
            pltpu.VMEM((count, lanes), F32),
            pltpu.VMEM((count, lanes), F32),
            pltpu.VMEM((4, max(count // BLOCK, 8), lanes), F32),
            pltpu.VMEM((ntp, count, part), BF16),
            pltpu.VMEM((count, features), BF16),
            pltpu.VMEM((3, n) + proj_state.shape, BF16),
            pltpu.VMEM((2, n) + merge_state.shape, BF16),
            pltpu.VMEM((count, width), BF16),
            pltpu.VMEM((count, 2 * lanes), F32),
            pltpu.VMEM((count, 2 * lanes), BF16),
            pltpu.VMEM((count + BLOCK, width), F32),
            pltpu.VMEM((count, width), F32),
            pltpu.VMEM((count, width), BF16),
            pltpu.VMEM((count, width), BF16),
            pltpu.VMEM((BLOCK, width), BF16),
            pltpu.VMEM((BLOCK, width), BF16),
            pltpu.VMEM((8, lanes // 2), F32),
            pltpu.VMEM((n, 8, lanes // 2), F32),
            pltpu.VMEM((8, count), F32),
            pltpu.VMEM((ntp, 8, count), F32),
            pieces, pieces, pieces, pieces, pieces,
            dma((6,)), dma((ny,)), dma((ny,)), dma((ny,)), dma((ny,)),
            dma((5, 2, hops)), dma((5, 2, hops)), dma, dma,
            dma((n,)), dma((n,)), dma((ntp,)), dma((ntp,)),
            dma((ny, quarters)), dma((ny, quarters)), dma((ny, quarters)), dma((ny, quarters)),
        ],
        compiler_params=pltpu.CompilerParams(
            collective_id=0, has_side_effects=True, vmem_limit_bytes=60 * 1024 * 1024
        ),
        name="mixer",
    )(
        tokens, norm_gain.reshape(1, features), proj_state, proj_value, proj_gate,
        eigen_real, eigen_imag, log_step.reshape(1, groups), decay_shift,
        state_input.reshape(2 * width, states), state_readout_matrices.reshape(2 * width, states),
        skip_gain.reshape(1, width), init_state.reshape(2 * groups, states), conv_taps,
        channel_gain.reshape(1, width), merge_state, merge_conv,
    )


def per_device_any(n, ntp, *args):
    tokens, merge_state = args[0], args[15]
    fits = (
        n % 8 == 0 and ntp % 2 == 0 and args[2].shape[0] % 128 == 0 and merge_state.shape[1] % 128 == 0
        and tokens.shape[0] % 128 == 0 and args[5].size % 256 == 0 and args[13].shape[0] <= BLOCK
    )
    if fits:
        return fused(n, ntp, *args)
    return per_device(*args)


def solution(mesh):
    return jax.shard_map(
        functools.partial(per_device_any, mesh.shape["sp"], mesh.shape["tp"]),
        mesh=mesh,
        in_specs=(
            P("sp", "tp"),
            P(),
            P("sp", "tp"),
            P("sp", "tp"),
            P("sp", "tp"),
            P("tp", None),
            P("tp", None),
            P("tp"),
            P("tp", "sp"),
            P(None, "tp", None, None),
            P(None, "tp", None, None),
            P("tp"),
            P(None, "tp", None),
            P(None, "tp"),
            P("tp"),
            P("tp", "sp"),
            P("tp", "sp"),
        ),
        out_specs=P(("sp", "tp"), None),
        check_vma=False,
    )
```

```python
import functools

import jax
import jax.numpy as jnp
from jax import lax
from jax.experimental import pallas as pl
from jax.experimental.pallas import tpu as pltpu
from jax.sharding import PartitionSpec as P

CONV_W = 1024


epsilon = 1e-06
exact_precision = lax.Precision.HIGHEST


def entering(value, axis, join, neutral):
    count, mine = (lax.axis_size(axis), lax.axis_index(axis))
    pieces = jax.tree.map(lambda part: lax.all_gather(part, axis), value)
    total = jax.tree.map(
        lambda part, zero: jnp.full_like(part, 0) + jnp.asarray(zero, part.dtype), value, neutral
    )

    def hop(position, total):
        longer = join(total, jax.tree.map(lambda part: part[position], pieces))
        return jax.tree.map(lambda new, old: jnp.where(position < mine, new, old), longer, total)

    return lax.fori_loop(0, count - 1, hop, total)


def passed_along(block, axis, distance):
    devices = range(lax.axis_size(axis))
    route = [(i - distance, i) for i in devices if i - distance in devices]
    return lax.ppermute(block, axis, route)


def round_half(value):
    return lax.optimization_barrier(value.astype(jnp.bfloat16))


def input_matrix(eigen_real, eigen_imag, step, state_input):
    base = eigen_real * step[:, None]
    theta = eigen_imag * step[:, None]
    magnitude = jnp.exp(base)
    near_re = magnitude * jnp.cos(theta) - 1.0
    near_im = magnitude * jnp.sin(theta)
    modulus = eigen_real * eigen_real + eigen_imag * eigen_imag
    ratio_re = (near_re * eigen_real + near_im * eigen_imag) / modulus
    ratio_im = (near_im * eigen_real - near_re * eigen_imag) / modulus
    in_re = state_input[0]
    in_im = state_input[1]
    discrete_decay_real = ratio_re[:, None, :] * in_re - ratio_im[:, None, :] * in_im
    discrete_decay_imaginary = ratio_re[:, None, :] * in_im + ratio_im[:, None, :] * in_re
    return (discrete_decay_real, discrete_decay_imaginary)


def block_states(c_re, c_im, delta_real, delta_imaginary, shift, base, theta, counts, lower):
    level = jnp.cumsum(shift, axis=0)[:, :, None] + counts * base
    angle = counts * theta
    cosine = jnp.cos(angle)
    sine = jnp.sin(angle)
    grow = jnp.exp(level)
    shrink = jnp.exp(-level)
    w_re = shrink * (cosine * delta_real + sine * delta_imaginary)
    w_im = shrink * (cosine * delta_imaginary - sine * delta_real)
    length, groups, states = delta_real.shape
    stacked = jnp.concatenate([w_re, w_im], axis=1).reshape(length, 2 * groups * states)
    summed = jnp.dot(lower, stacked, precision=exact_precision).reshape(length, 2 * groups, states)
    t_re = summed[:, :groups] + c_re
    t_im = summed[:, groups:] + c_im
    input_real = grow * (cosine * t_re - sine * t_im)
    input_imaginary = grow * (cosine * t_im + sine * t_re)
    return (input_real, input_imaginary)


def chain(earlier, later):
    a_re, a_im, b_re, b_im = earlier
    c_re, c_im, delta_real, delta_imaginary = later
    return (
        a_re * c_re - a_im * c_im,
        a_re * c_im + a_im * c_re,
        c_re * b_re - c_im * b_im + delta_real,
        c_re * b_im + c_im * b_re + delta_imaginary,
    )


def state_local(
    u_in, eigen_real, eigen_imag, log_step, decay_shift, state_input, state_readout_matrices
):
    count, width = u_in.shape
    groups, states = eigen_real.shape
    group = width // groups
    step = jnp.exp(log_step)
    base = eigen_real * step[:, None]
    theta = eigen_imag * step[:, None]
    discrete_decay_real, discrete_decay_imaginary = input_matrix(
        eigen_real, eigen_imag, step, state_input
    )
    float_values = u_in.astype(jnp.float32).reshape(count, groups, group)
    forcing_real = jnp.einsum(
        "ovi,viu->ovu", float_values, discrete_decay_real, precision=exact_precision
    )
    forcing_imaginary = jnp.einsum(
        "ovi,viu->ovu", float_values, discrete_decay_imaginary, precision=exact_precision
    )
    shift = decay_shift.T
    length = min(32, count)
    blocks = count // length
    counts = (jnp.arange(length) + 1).astype(jnp.float32)[:, None, None]
    lower = (jnp.arange(length)[:, None] >= jnp.arange(length)[None, :]).astype(jnp.float32)

    def advance(carry, inputs):
        delta_real, delta_imaginary, block_shift = inputs
        input_real, input_imaginary = block_states(
            carry[0], carry[1], delta_real, delta_imaginary, block_shift, base, theta, counts, lower
        )
        return ((input_real[-1], input_imaginary[-1]), (input_real, input_imaginary))

    zero = jnp.zeros((groups, states), jnp.float32)
    last, (input_real, input_imaginary) = lax.scan(
        advance,
        (zero, zero),
        (
            forcing_real.reshape(blocks, length, groups, states),
            forcing_imaginary.reshape(blocks, length, groups, states),
            shift.reshape(blocks, length, groups),
        ),
    )
    input_real = input_real.reshape(count, groups, states)
    input_imaginary = input_imaginary.reshape(count, groups, states)
    local_output = jnp.einsum(
        "lan,arn->lar", input_real, state_readout_matrices[0], precision=exact_precision
    ) - jnp.einsum(
        "lan,arn->lar", input_imaginary, state_readout_matrices[1], precision=exact_precision
    )
    whole_count = (jnp.arange(count) + 1).astype(jnp.float32)[:, None, None]
    level = jnp.cumsum(shift, axis=0)[:, :, None] + whole_count * base
    angle = whole_count * theta
    grow = jnp.exp(level)
    exponent_real = grow * jnp.cos(angle)
    exponent_imaginary = grow * jnp.sin(angle)
    summary = (exponent_real[-1], exponent_imaginary[-1], last[0], last[1])
    return (local_output, exponent_real, exponent_imaginary, summary)


def carry_in(summary, init_state):
    groups, states = summary[0].shape
    ones = jnp.ones((groups, states), jnp.float32)
    zeros = jnp.zeros((groups, states), jnp.float32)
    identity = (ones, zeros, zeros, zeros)
    before = entering(summary, "sp", chain, identity)
    a_re, a_im, b_re, b_im = before
    s_re = init_state[0]
    s_im = init_state[1]
    return (a_re * s_re - a_im * s_im + b_re, a_re * s_im + a_im * s_re + b_im)


def state_finish(
    local_output,
    exponent_real,
    exponent_imaginary,
    carried,
    state_readout_matrices,
    skip_gain,
    u_in,
):
    h_re, h_im = carried
    output_real = state_readout_matrices[0]
    output_imaginary = state_readout_matrices[1]
    blend_real = output_real * h_re[:, None, :] - output_imaginary * h_im[:, None, :]
    blend_imaginary = output_real * h_im[:, None, :] + output_imaginary * h_re[:, None, :]
    total = (
        local_output
        + jnp.einsum("lan,arn->lar", exponent_real, blend_real, precision=exact_precision)
        - jnp.einsum("lan,arn->lar", exponent_imaginary, blend_imaginary, precision=exact_precision)
    )
    count, width = u_in.shape
    groups = local_output.shape[1]
    float_values = u_in.astype(jnp.float32).reshape(count, groups, width // groups)
    total = total + skip_gain.reshape(groups, width // groups) * float_values
    return jax.nn.gelu(total).reshape(count, width).astype(jnp.bfloat16)


def conv_branch(value, gate, conv_taps, channel_gain):
    glu = round_half(value.astype(jnp.float32) * jax.nn.sigmoid(gate.astype(jnp.float32)))
    reach = conv_taps.shape[0] - 1
    count = glu.shape[0]
    before = passed_along(glu[count - reach :], "sp", 1)
    extended = jnp.concatenate([before, glu], axis=0).astype(jnp.float32)
    raw = jnp.zeros(glu.shape, jnp.float32)
    for offset in range(reach + 1):
        raw = raw + conv_taps[offset] * extended[offset : offset + count]
    first, second = lax.psum(
        (jnp.sum(raw, axis=1, keepdims=True), jnp.sum(raw * raw, axis=1, keepdims=True)), "tp"
    )
    middle = first / CONV_W
    spread = second / CONV_W - middle * middle
    scaled = (raw - middle) * lax.rsqrt(spread + epsilon) * channel_gain
    return jax.nn.silu(scaled).astype(jnp.bfloat16)


def per_device(
    tokens,
    norm_gain,
    proj_state,
    proj_value,
    proj_gate,
    eigen_real,
    eigen_imag,
    log_step,
    decay_shift,
    state_input,
    state_readout_matrices,
    skip_gain,
    init_state,
    conv_taps,
    channel_gain,
    merge_state,
    merge_conv,
):
    whole = lax.all_gather(tokens, "tp", axis=1, tiled=True)
    wide = whole.astype(jnp.float32)
    normed = (
        wide * lax.rsqrt(jnp.mean(wide * wide, axis=1, keepdims=True) + epsilon) * norm_gain
    ).astype(jnp.bfloat16)
    pieces = (
        lax.all_gather(proj_state, "sp", axis=0, tiled=True),
        lax.all_gather(proj_value, "sp", axis=0, tiled=True),
        lax.all_gather(proj_gate, "sp", axis=0, tiled=True),
    )
    state_sum, value_sum, gate_sum = tuple(
        (jnp.dot(normed, piece, preferred_element_type=jnp.float32) for piece in pieces)
    )
    u_in = round_half(state_sum)
    local_output, exponent_real, exponent_imaginary, summary = state_local(
        u_in, eigen_real, eigen_imag, log_step, decay_shift, state_input, state_readout_matrices
    )
    carried = carry_in(summary, init_state)
    conv_out = conv_branch(round_half(value_sum), round_half(gate_sum), conv_taps, channel_gain)
    ssm_out = state_finish(
        local_output,
        exponent_real,
        exponent_imaginary,
        carried,
        state_readout_matrices,
        skip_gain,
        u_in,
    )
    full_state, full_conv = (
        lax.all_gather(merge_state, "sp", axis=1, tiled=True),
        lax.all_gather(merge_conv, "sp", axis=1, tiled=True),
    )
    return lax.psum_scatter(
        (
            jnp.dot(ssm_out, full_state, preferred_element_type=jnp.float32)
            + jnp.dot(conv_out, full_conv, preferred_element_type=jnp.float32)
        ).astype(jnp.bfloat16),
        "tp",
        scatter_dimension=0,
        tiled=True,
    )


MESH = pl.DeviceIdType.MESH
F32 = jnp.float32
BF16 = jnp.bfloat16
BLOCK = 32


def dot(a, b):
    return jnp.dot(a, b, preferred_element_type=F32)


def dot_exact(a, b):
    return jnp.dot(a, b, preferred_element_type=F32, precision=exact_precision)


def split(value):
    high = value.astype(BF16)
    return high, (value - high.astype(F32)).astype(BF16)


def ring_position(index, n):
    return jnp.where(index % 2 == 0, index // 2, n - 1 - index // 2)


def ring_index(position, n):
    position = lax.rem(position + 2 * n, n)
    return jnp.where(position < n // 2, 2 * position, 2 * (n - 1 - position) + 1)


def mixer_kernel(
    n, ntp,
    tokens, gain, proj_s, proj_v, proj_g, eig_re, eig_im, log_step, decay,
    state_in, state_out, skip, init, taps, chgain, merge_s, merge_c,
    out,
    shift, base_t, cos_t, sin_t, bin_high, bin_low, cout, into_re, into_im, back_re, back_im, held,
    tok, normed, gat, mgat, u_buf, forc, xs, ext, raw, ssm, conv,
    halo, glu_tail, summ, summ_in, stat, stat_in, snd, own, rp, s2, r2,
    loc_sem, tok_s, tok_r, fwd_s, fwd_r, ring_s, ring_r, halo_s, halo_r,
    sum_s, sum_r, st_s, st_r, rp_s, rp_r, r2_s, r2_r,
):
    sp = lax.axis_index("sp")
    tp = lax.axis_index("tp")
    ny = ntp // 2
    y, core = tp // 2, tp % 2
    partner = y * 2 + 1 - core
    pos = ring_position(sp, n)
    right, left = ring_index(pos + 1, n), ring_index(pos - 1, n)
    count, width = u_buf.shape
    groups, states = eig_re.shape
    lanes = groups * states
    part = tokens.shape[1]
    rows_w = proj_s.shape[0]

    halo[...] = jnp.zeros_like(halo)
    summ_in[...] = jnp.zeros_like(summ_in)

    barrier = pltpu.get_barrier_semaphore()
    for d in range(1, n):
        pl.semaphore_signal(barrier, inc=1, device_id=(lax.rem(sp + d, n), tp), device_id_type=MESH)
    for d in range(1, ntp):
        pl.semaphore_signal(barrier, inc=1, device_id=(sp, lax.rem(tp + d, ntp)), device_id_type=MESH)
    pl.semaphore_wait(barrier, n + ntp - 2)

    def remote(src, dst, s, r, where):
        return pltpu.make_async_remote_copy(
            src_ref=src, dst_ref=dst, send_sem=s, recv_sem=r, device_id=where, device_id_type=MESH
        )

    sources = (proj_s, proj_v, proj_g, merge_s, merge_c)
    hops = n // 2

    def slot(w, origin):
        return gat.at[w, origin] if w < 3 else mgat.at[w - 3, origin]

    def piece(w, side, step):
        origin = ring_index(pos - step if side == 0 else pos + step, n)
        where = (right if side == 0 else left, tp)
        src = sources[w] if step == 0 else slot(w, origin)
        dst = slot(w, origin)
        if step == hops - 1:
            half = src.shape[0] // 2
            window = pl.ds(side * half, half)
            src, dst = src.at[window], dst.at[window]
        return remote(src, dst, ring_s.at[w, side, step], ring_r.at[w, side, step], where)

    def ring_send(ws, step):
        for w in ws:
            for side in range(2):
                if step > 0:
                    piece(w, side, step - 1).wait_recv()
                piece(w, side, step).start()

    def ring_end(ws):
        for w in ws:
            for side in range(2):
                piece(w, side, hops - 1).wait_recv()

    ring_send([0, 1], 0)

    def tok_copy(d):
        where = (sp, lax.rem(y + d, ny) * 2 + core) if d else (sp, partner)
        return remote(tokens, tok.at[tp], tok_s.at[d], tok_r.at[d], where)

    def tok_forward(d):
        origin = lax.rem(y - d + ny, ny) * 2 + core
        return remote(tok.at[origin], tok.at[origin], fwd_s.at[d], fwd_r.at[d], (sp, partner))

    for d in list(range(1, ny)) + [0]:
        tok_copy(d).start()
    local = [pltpu.make_async_copy(tokens, tok.at[tp], loc_sem.at[5])]
    for w in range(5):
        local.append(pltpu.make_async_copy(sources[w], slot(w, sp), loc_sem.at[w]))
    for c in local:
        c.start()

    row_i = lax.broadcasted_iota(jnp.int32, (BLOCK, BLOCK), 0)
    col_i = lax.broadcasted_iota(jnp.int32, (BLOCK, BLOCK), 1)
    lower = (row_i >= col_i).astype(F32)
    last = slice(BLOCK - 1, BLOCK)

    def lane_of(rows):
        return lax.broadcasted_iota(jnp.int32, (rows, lanes), 1)

    def row_of(rows):
        return lax.broadcasted_iota(jnp.int32, (rows, lanes), 0)

    repeat = (lax.rem(lane_of(states), states) == row_of(states)).astype(F32)
    mine = lax.div(lane_of(groups), states) == row_of(groups)
    expand = mine.astype(F32)

    def to_row(matrix):
        return jnp.sum(jnp.where(mine, dot_exact(matrix, repeat), 0.0), axis=0, keepdims=True)

    square_row = lax.broadcasted_iota(jnp.int32, (groups, groups), 0)
    square_col = lax.broadcasted_iota(jnp.int32, (groups, groups), 1)
    steps = jnp.broadcast_to(jnp.exp(log_step[...]), (groups, groups))
    step_size = jnp.sum(jnp.where(square_row == square_col, steps, 0.0), axis=1, keepdims=True)
    real_row, imag_row = to_row(eig_re[...]), to_row(eig_im[...])
    base_row = to_row(eig_re[...] * step_size)
    theta_row = to_row(eig_im[...] * step_size)
    counts = (row_of(BLOCK) + 1).astype(F32)
    base_t[...] = counts * base_row
    cos_t[...] = jnp.cos(counts * theta_row)
    sin_t[...] = jnp.sin(counts * theta_row)
    magnitude = jnp.exp(base_row)
    near_re = magnitude * cos_t[0:1, :] - 1.0
    near_im = magnitude * sin_t[0:1, :]
    modulus = real_row * real_row + imag_row * imag_row
    ratio_re = (near_re * real_row + near_im * imag_row) / modulus
    ratio_im = (near_im * real_row - near_re * imag_row) / modulus
    group = width // groups
    chunk = 256
    for j in range(lanes // chunk):
        cols = slice(j * chunk, (j + 1) * chunk)
        later = slice(lanes + j * chunk, lanes + (j + 1) * chunk)
        spot = lax.broadcasted_iota(jnp.int32, (width, chunk), 1) + j * chunk
        whose = lax.div(lax.broadcasted_iota(jnp.int32, (width, chunk), 0), group)
        same = lax.div(spot, states) == whose
        m_re = dot_exact(state_in[0:width, :], repeat[:, cols])
        m_im = dot_exact(state_in[width : 2 * width, :], repeat[:, cols])
        r_re, r_im = ratio_re[:, cols], ratio_im[:, cols]
        bin_high[:, cols], bin_low[:, cols] = split(jnp.where(same, r_re * m_re - r_im * m_im, 0.0))
        bin_high[:, later], bin_low[:, later] = split(jnp.where(same, r_re * m_im + r_im * m_re, 0.0))
        m_re = dot_exact(state_out[0:width, :], repeat[:, cols])
        m_im = dot_exact(state_out[width : 2 * width, :], repeat[:, cols])
        cout[:, cols] = jnp.where(same, m_re, 0.0).astype(BF16)
        cout[:, later] = jnp.where(same, -m_im, 0.0).astype(BF16)
    start_re, start_im = to_row(init[0:groups, :]), to_row(init[groups : 2 * groups, :])
    fill_rows = jnp.zeros((128 - groups, count), F32)
    shift[...] = jnp.concatenate([decay[...], fill_rows], axis=0).T

    ring_send([0, 1], 1)

    def prepare(k, state):
        a_re, a_im = state
        rows = pl.ds(pl.multiple_of(k * BLOCK, BLOCK), BLOCK)
        level = dot_exact(dot_exact(lower, shift[rows, :])[:, :groups], expand) + base_t[...]
        grow, shrink = jnp.exp(level), jnp.exp(-level)
        cosine, sine = cos_t[...], sin_t[...]
        into_re[rows, :] = shrink * cosine
        into_im[rows, :] = shrink * sine
        g_re, g_im = grow * cosine, grow * sine
        back_re[rows, :] = g_re
        back_im[rows, :] = g_im
        held[0, pl.ds(k, 1), :] = a_re
        held[1, pl.ds(k, 1), :] = a_im
        e_re, e_im = g_re[last], g_im[last]
        return a_re * e_re - a_im * e_im, a_re * e_im + a_im * e_re

    zero = jnp.zeros((1, lanes), F32)
    blocks = count // BLOCK
    decayed = lax.fori_loop(0, blocks // 2, prepare, (zero + 1.0, zero))
    ring_send([0, 1], 2)
    for d in range(1, ny):
        tok_copy(d).wait_recv()
        tok_forward(d).start()
    decayed = lax.fori_loop(blocks // 2, blocks, prepare, decayed)
    for step in range(3, hops - 1):
        ring_send([0, 1], step)
    ring_send([0], hops - 1)
    ring_send([2], 0)
    ring_send([1], hops - 1)
    ring_send([3], 0)
    tok_copy(0).wait_recv()
    for c in local:
        c.wait()
    for d in range(1, ny):
        tok_forward(d).wait_recv()

    tile = 64

    @pl.loop(0, count // tile)
    def _(i):
        rows = pl.ds(pl.multiple_of(i * tile, tile), tile)
        pieces = [tok[j, rows, :].astype(F32) for j in range(ntp)]
        square = sum(jnp.sum(p * p, axis=1, keepdims=True) for p in pieces)
        scale = lax.rsqrt(square / (part * ntp) + epsilon)
        for j in range(ntp):
            cols = slice(j * part, (j + 1) * part)
            normed[rows, cols] = (pieces[j] * scale * gain[:, cols]).astype(BF16)

    ring_end([0])

    big = 128

    def project(w, i):
        rows = pl.ds(pl.multiple_of(i * big, big), big)
        total = dot(normed[rows, 0:rows_w], gat[w, 0])
        for o in range(1, n):
            total += dot(normed[rows, o * rows_w : (o + 1) * rows_w], gat[w, o])
        return rows, total.astype(BF16)

    @pl.loop(0, count // big)
    def _(i):
        rows, u = project(0, i)
        u_buf[rows, :] = u

    ring_send([2], 1)
    ring_send([4], 0)

    wide = 256

    @pl.loop(0, 2 * lanes // wide)
    def _(j):
        cols = pl.ds(pl.multiple_of(j * wide, wide), wide)
        forc[:, cols] = dot(u_buf[...], bin_high[:, cols]) + dot(u_buf[...], bin_low[:, cols])

    def first_pass(k, state):
        c_re, c_im = state
        rows = pl.ds(pl.multiple_of(k * BLOCK, BLOCK), BLOCK)
        held[2, pl.ds(k, 1), :] = c_re
        held[3, pl.ds(k, 1), :] = c_im
        d_re, d_im = forc[rows, :lanes], forc[rows, lanes:]
        w_re = into_re[rows, :] * d_re + into_im[rows, :] * d_im
        w_im = into_re[rows, :] * d_im - into_im[rows, :] * d_re
        forc[rows, :lanes] = w_re
        forc[rows, lanes:] = w_im
        final = pl.ds(k * BLOCK + BLOCK - 1, 1)
        e_re, e_im = back_re[final, :], back_im[final, :]
        t_re = c_re + jnp.sum(w_re, axis=0, keepdims=True)
        t_im = c_im + jnp.sum(w_im, axis=0, keepdims=True)
        return e_re * t_re - e_im * t_im, e_re * t_im + e_im * t_re

    ended = lax.fori_loop(0, blocks // 2, first_pass, (zero, zero), unroll=2)
    ring_send([2], 2)
    ring_send([3], 1)
    ended = decayed + lax.fori_loop(blocks // 2, blocks, first_pass, ended, unroll=2)
    half = lanes // 2
    for r in range(4):
        summ[r : r + 1, :] = ended[r][:, :half]
        summ[4 + r : 5 + r, :] = ended[r][:, half:]

    def summ_copy(d):
        return remote(summ, summ_in.at[sp], sum_s.at[d], sum_r.at[d], (lax.rem(sp + d, n), tp))

    for d in range(1, n):

        @pl.when(sp + d < n)
        def _():
            summ_copy(d).start()


    for d in range(1, n):

        @pl.when(sp >= d)
        def _():
            summ_copy(d).wait_recv()

    def unpack(block):
        return [jnp.concatenate([block[r : r + 1], block[4 + r : 5 + r]], axis=1) for r in range(4)]

    h_re, h_im = start_re, start_im
    for q in range(n - 1):
        a_re, a_im, b_re, b_im = unpack(summ_in[q])
        n_re = a_re * h_re - a_im * h_im + b_re
        n_im = a_re * h_im + a_im * h_re + b_im
        h_re = jnp.where(q < sp, n_re, h_re)
        h_im = jnp.where(q < sp, n_im, h_im)

    lower_half = lower.astype(BF16)

    def second_pass(k, _):
        rows = pl.ds(pl.multiple_of(k * BLOCK, BLOCK), BLOCK)
        one = pl.ds(k, 1)
        a_re, a_im = held[0, one, :], held[1, one, :]
        c_re = held[2, one, :] + a_re * h_re - a_im * h_im
        c_im = held[3, one, :] + a_re * h_im + a_im * h_re
        high, low = split(forc[rows, :])
        summed = dot(lower_half, high) + dot(lower_half, low)
        t_re = summed[:, :lanes] + c_re
        t_im = summed[:, lanes:] + c_im
        g_re, g_im = back_re[rows, :], back_im[rows, :]
        xs[rows, :lanes] = (g_re * t_re - g_im * t_im).astype(BF16)
        xs[rows, lanes:] = (g_re * t_im + g_im * t_re).astype(BF16)
        return 0

    lax.fori_loop(0, blocks // 2, second_pass, 0, unroll=2)
    for step in range(3, hops - 1):
        ring_send([2], step)
    ring_send([2], hops - 1)
    ring_send([4], 1)
    lax.fori_loop(blocks // 2, blocks, second_pass, 0, unroll=2)
    ring_send([3], 2)
    ring_end([1, 2])

    @pl.loop(0, count // big)
    def _(i):
        rows, value = project(1, i)
        rows, gate = project(2, i)
        glu = (value.astype(F32) * jax.nn.sigmoid(gate.astype(F32))).astype(BF16)
        ext[pl.ds(pl.multiple_of(BLOCK + i * big, BLOCK), big), :] = glu.astype(F32)

    glu_tail[...] = ext[count : count + BLOCK, :].astype(BF16)
    halo_to = lax.rem(sp + 1, n)
    halo_copy = remote(glu_tail, halo, halo_s, halo_r, (halo_to, tp))

    @pl.when(sp < n - 1)
    def _():
        halo_copy.start()

    reach = taps.shape[0] - 1
    ring_send([4], 2)
    for step in range(3, hops - 1):
        ring_send([3, 4], step)

    def taps_on(start):
        window = ext[pl.ds(start, tile + BLOCK), :]
        total = jnp.zeros((tile, width), F32)
        for k in range(reach + 1):
            at = BLOCK - reach + k
            total += taps[k : k + 1, :] * window[at : at + tile, :]
        raw[pl.ds(start, tile), :] = total

    @pl.loop(1, count // tile)
    def _(i):
        taps_on(pl.multiple_of(i * tile, tile))

    @pl.when(sp > 0)
    def _():
        halo_copy.wait_recv()

    ext[0:BLOCK, :] = halo[...].astype(F32)
    taps_on(0)

    lane = lax.broadcasted_iota(jnp.int32, (count, 128), 1)
    values = raw[...]
    first = jnp.sum(values, axis=1, keepdims=True)
    second = jnp.sum(values * values, axis=1, keepdims=True)
    packed = jnp.where(lane == 0, first, jnp.where(lane == 1, second, 0.0))
    stat[...] = packed.T[0:8, :]

    def stat_copy(d):
        return remote(stat, stat_in.at[d], st_s.at[d], st_r.at[d], (sp, lax.rem(tp + d, ntp)))

    for d in range(1, ntp):
        stat_copy(d).start()
    ring_send([3, 4], hops - 1)

    @pl.loop(0, count // big)
    def _(i):
        rows = pl.ds(pl.multiple_of(i * big, big), big)
        total = lax.dot_general(
            xs[rows, :], cout[...], (((1,), (1,)), ((), ())), preferred_element_type=F32
        )
        total += skip[...] * u_buf[rows, :].astype(F32)
        ssm[rows, :] = jax.nn.gelu(total).astype(BF16)

    for d in range(1, ntp):
        stat_copy(d).wait_recv()
    sums = stat[...]
    for d in range(1, ntp):
        sums += stat_in[d]
    channels = width * ntp
    middle_row = sums[0:1] / channels
    inverse_row = lax.rsqrt(sums[1:2] / channels - middle_row * middle_row + epsilon)
    row = lax.broadcasted_iota(jnp.int32, (128, count), 0)
    columns = jnp.where(row == 0, middle_row, inverse_row).T
    scaled = (raw[...] - columns[:, 0:1]) * columns[:, 1:2] * chgain[...]
    conv[...] = jax.nn.silu(scaled).astype(BF16)

    ring_end([3, 4])
    quarters, block_rows = snd.shape[1], snd.shape[2]
    per = n // quarters
    cw = merge_s.shape[1]

    def product(block, q):
        rows = pl.ds(pl.multiple_of(block * block_rows, block_rows), block_rows)
        a, b = ssm[rows, :], conv[rows, :]
        outs = []
        for o in range(q * per, (q + 1) * per):
            outs.append((dot(a, mgat[0, o]) + dot(b, mgat[1, o])).astype(BF16))
        return outs

    def to_partner(d, q):
        return remote(snd.at[d, q], rp.at[d, q], rp_s.at[d, q], rp_r.at[d, q], (sp, partner))

    def across(d, q):
        where = (sp, lax.rem(y + d, ny) * 2 + core)
        return remote(s2.at[d, q], r2.at[d, q], r2_s.at[d, q], r2_r.at[d, q], where)

    order = list(range(1, ny)) + [0]

    def fill(buffer, d, q, which):
        for i, value in enumerate(product(lax.rem(y + d, ny) * 2 + which, q)):
            buffer[d, q, :, i * cw : (i + 1) * cw] = value

    def relay(d, q):
        to_partner(d, q).wait_recv()
        s2[d, q] = (own[d, q].astype(F32) + rp[d, q].astype(F32)).astype(BF16)
        across(d, q).start()

    for d in order:
        for q in range(quarters):
            fill(snd, d, q, 1 - core)
            to_partner(d, q).start()
            fill(own, d, q, core)
            if d and q:
                relay(d, q - 1)
        if d:
            relay(d, quarters - 1)
    for q in range(quarters):
        to_partner(0, q).wait_recv()
        total = own[0, q].astype(F32) + rp[0, q].astype(F32)
        for d in range(1, ny):
            across(d, q).wait_recv()
            total += r2[d, q].astype(F32)
        out[:, q * per * cw : (q + 1) * per * cw] = total.astype(BF16)

    for w in range(5):
        for side in range(2):
            for step in range(hops):
                piece(w, side, step).wait_send()
    for d in range(ny):
        tok_copy(d).wait_send()
        if d:
            tok_forward(d).wait_send()
        for q in range(quarters):
            to_partner(d, q).wait_send()
            if d:
                across(d, q).wait_send()
    for d in range(1, ntp):
        stat_copy(d).wait_send()

    @pl.when(sp < n - 1)
    def _():
        halo_copy.wait_send()

    for d in range(1, n):

        @pl.when(sp + d < n)
        def _():
            summ_copy(d).wait_send()


def fused(
    n, ntp, tokens, norm_gain, proj_state, proj_value, proj_gate, eigen_real, eigen_imag,
    log_step, decay_shift, state_input, state_readout_matrices, skip_gain, init_state,
    conv_taps, channel_gain, merge_state, merge_conv,
):
    count, part = tokens.shape
    groups, states = eigen_real.shape
    width = proj_state.shape[1]
    lanes = groups * states
    features = part * ntp
    quarters = min(4, n)
    ny = ntp // 2
    block_rows = count // ntp
    cw = merge_state.shape[1] * n // quarters
    pieces = pltpu.VMEM((ny, quarters, block_rows, cw), BF16)
    vmem = pl.BlockSpec(memory_space=pltpu.VMEM)
    hops = n // 2
    dma = pltpu.SemaphoreType.DMA
    return pl.pallas_call(
        functools.partial(mixer_kernel, n, ntp),
        out_shape=jax.ShapeDtypeStruct((block_rows, features), BF16),
        in_specs=[vmem] * 17,
        out_specs=vmem,
        scratch_shapes=[
            pltpu.VMEM((count, 128), F32),
            pltpu.VMEM((BLOCK, lanes), F32),
            pltpu.VMEM((BLOCK, lanes), F32),
            pltpu.VMEM((BLOCK, lanes), F32),
            pltpu.VMEM((width, 2 * lanes), BF16),
            pltpu.VMEM((width, 2 * lanes), BF16),
            pltpu.VMEM((width, 2 * lanes), BF16),
            pltpu.VMEM((count, lanes), F32),
            pltpu.VMEM((count, lanes), F32),
            pltpu.VMEM((count, lanes), F32),
            pltpu.VMEM((count, lanes), F32),
            pltpu.VMEM((4, max(count // BLOCK, 8), lanes), F32),
            pltpu.VMEM((ntp, count, part), BF16),
            pltpu.VMEM((count, features), BF16),
            pltpu.VMEM((3, n) + proj_state.shape, BF16),
            pltpu.VMEM((2, n) + merge_state.shape, BF16),
            pltpu.VMEM((count, width), BF16),
            pltpu.VMEM((count, 2 * lanes), F32),
            pltpu.VMEM((count, 2 * lanes), BF16),
            pltpu.VMEM((count + BLOCK, width), F32),
            pltpu.VMEM((count, width), F32),
            pltpu.VMEM((count, width), BF16),
            pltpu.VMEM((count, width), BF16),
            pltpu.VMEM((BLOCK, width), BF16),
            pltpu.VMEM((BLOCK, width), BF16),
            pltpu.VMEM((8, lanes // 2), F32),
            pltpu.VMEM((n, 8, lanes // 2), F32),
            pltpu.VMEM((8, count), F32),
            pltpu.VMEM((ntp, 8, count), F32),
            pieces, pieces, pieces, pieces, pieces,
            dma((6,)), dma((ny,)), dma((ny,)), dma((ny,)), dma((ny,)),
            dma((5, 2, hops)), dma((5, 2, hops)), dma, dma,
            dma((n,)), dma((n,)), dma((ntp,)), dma((ntp,)),
            dma((ny, quarters)), dma((ny, quarters)), dma((ny, quarters)), dma((ny, quarters)),
        ],
        compiler_params=pltpu.CompilerParams(
            collective_id=0, has_side_effects=True, vmem_limit_bytes=60 * 1024 * 1024
        ),
        name="mixer",
    )(
        tokens, norm_gain.reshape(1, features), proj_state, proj_value, proj_gate,
        eigen_real, eigen_imag, log_step.reshape(1, groups), decay_shift,
        state_input.reshape(2 * width, states), state_readout_matrices.reshape(2 * width, states),
        skip_gain.reshape(1, width), init_state.reshape(2 * groups, states), conv_taps,
        channel_gain.reshape(1, width), merge_state, merge_conv,
    )


def per_device_any(n, ntp, *args):
    tokens, merge_state = args[0], args[15]
    fits = (
        n % 8 == 0 and ntp % 2 == 0 and args[2].shape[0] % 128 == 0 and merge_state.shape[1] % 128 == 0
        and tokens.shape[0] % 128 == 0 and args[5].size % 256 == 0 and args[13].shape[0] <= BLOCK
    )
    if fits:
        return fused(n, ntp, *args)
    return per_device(*args)


def solution(mesh):
    return jax.shard_map(
        functools.partial(per_device_any, mesh.shape["sp"], mesh.shape["tp"]),
        mesh=mesh,
        in_specs=(
            P("sp", "tp"),
            P(),
            P("sp", "tp"),
            P("sp", "tp"),
            P("sp", "tp"),
            P("tp", None),
            P("tp", None),
            P("tp"),
            P("tp", "sp"),
            P(None, "tp", None, None),
            P(None, "tp", None, None),
            P("tp"),
            P(None, "tp", None),
            P(None, "tp"),
            P("tp"),
            P("tp", "sp"),
            P("tp", "sp"),
        ),
        out_specs=P(("sp", "tp"), None),
        check_vma=False,
    )
```
